32 devices in a mesh: sp: 4 (over y, x), tp: 8 (over z, core).
Axes of the slice: x: 2, y: 2, z: 4, core: 2. Of those that a mesh axis runs over, the one named last changes fastest.
Arguments:
- queries: bfloat16 [1536, 2048], P('sp', 'tp'), may hold values from -6 to 6
- cell_key_rows: bfloat16 [1536, 2048], P('sp', 'tp'), may hold values from -6 to 6
- cell_value_rows: bfloat16 [1536, 2048], P('sp', 'tp'), may hold values from -6 to 6
- output_gate_logits: bfloat16 [1536, 2048], P('sp', 'tp'), may hold values from -6 to 6
- input_gate_logs: float32 [16, 1536], P('tp', 'sp'), may hold values from -5 to 250
- forget_gate_logits: float32 [16, 1536], P('tp', 'sp'), may hold values from 1 to 13
- extra_log_forget: float32 [16, 1536], P('tp', 'sp'), may hold values from -0.7 to 0
- head_norm_gain: float32 [2048], P('tp'), may hold values from 0.1 to 1.9
- cell_output_matrix: bfloat16 [2048, 4096], P('tp'), may hold values from -0.125 to 0.125
- residual: bfloat16 [1536, 4096], P('sp'), may hold values from -6 to 6
- expert_norm_gain: float32 [4096], replicated, may hold values from 0.1 to 1.9
- routes: int32 [1536, 2], P('sp'), may hold values from 0 to 3, all different within a row; in each aligned block of 48 rows (0 to 47, 48 to 95, ...) at most 48 rows name the same one
- token_expert_weights: float32 [1536, 2], P('sp'), may hold values from 0.2 to 1
- expert_gate_matrix: bfloat16 [4, 4096, 2048], P('sp', None, 'tp'), may hold values from -0.09375 to 0.09375
- expert_up_matrix: bfloat16 [4, 4096, 2048], P('sp', None, 'tp'), may hold values from -0.09375 to 0.09375
- expert_down_matrix: bfloat16 [4, 2048, 4096], P('sp', 'tp'), may hold values from -0.125 to 0.125
Outputs:
- layer_out: bfloat16 [1536, 4096], P(('sp', 'tp'))
The draws below stay inside these ranges and needn't reach their ends.
Inputs may be any that keep to these rules, and one draw needn't show every extreme that they name: `routes`: each row names 2 different experts. In the rows of one device (aligned blocks of 48 rows) no expert is named more than 48 times, and in some blocks one expert is named exactly 48 times.
All inputs are finite; a program needn't handle non-finite values.
Results may differ from the reference program's by a relative error of at most 0.019.
Values may be sent and summed in bfloat16 or wider, within the bound.
A program may use at most 128 MiB of HBM per device.

```python
import math
import jax
import jax.numpy as jnp
import numpy as np
from jax import lax

D = 4096
HEADS = 16
HEAD_DIM = 128
MIX = 2048
FF = 2048
EXPERTS = 4
TOPK = 2
S_DEV = 384
SEQ = 1536
TOK_DEV = 48
CAP = 48
BLOCK = 128
N_TP = 8


def draw_forget_gate_logits(key, part):
    slow_key, shift_key, noise_key = jax.random.split(jax.random.fold_in(key, 11), 3)
    pick = jax.random.uniform(slow_key, (HEADS, 1))
    slow = pick < 0.5
    noise = 0.5 * jnp.clip(jax.random.normal(noise_key, (HEADS, SEQ)), -3.0, 3.0)
    base = jnp.where(slow, jnp.log(2.0 * SEQ), jnp.log(40.0))
    shifts = jax.random.uniform(shift_key, (HEADS, SEQ // S_DEV), minval=-1.0, maxval=1.0)
    return (base + jnp.repeat(shifts, S_DEV, axis=1) + noise).astype(jnp.float32)


def draw_input_gate_logs(key, part):
    base_key = jax.random.fold_in(jax.random.fold_in(key, 13), 0)
    values = jnp.clip(jax.random.normal(base_key, (HEADS, SEQ)), -5.0, 5.0)
    return values.astype(jnp.float32)


def draw_extra_log_forget(key, part):
    place_key, size_key = jax.random.split(jax.random.fold_in(key, 17), 2)
    planted = jax.random.uniform(place_key, (HEADS, SEQ)) < 3.0 / SEQ
    sizes = jnp.log(jax.random.uniform(size_key, (HEADS, SEQ), minval=0.5, maxval=0.8))
    return jnp.where(planted, sizes, 0.0).astype(jnp.float32)


def block_levels(stream_key, shape, shards, least, top_value):
    loudness = 1.0
    for position, shards_of in shards:
        steps = jax.random.uniform(jax.random.fold_in(jax.random.fold_in(stream_key, 6), position), (shards_of,), jnp.float32, least / len(shards), top_value / len(shards))
        loudness = loudness * jnp.repeat(jnp.exp(steps), shape[position] // shards_of).reshape((-1,) + (1,) * (len(shape) - 1 - position))
    return loudness


def assign_block(rng, own, number, rows, amount, top, most, lean):
    order = jax.random.permutation(rng, amount)
    heavy_load, usual = load_shares(amount, rows * top, most, lean, True), load_shares(amount, rows * top, most, lean, False)
    places = jnp.arange(amount)

    def named(tallies, rotation):
        used = int((tallies > 0).sum())
        fixed = max(1, used // 4)
        passed = fixed + (places - fixed + rotation * (used - fixed)) % max(1, amount - fixed)
        return jnp.zeros((amount,), jnp.int32).at[order[jnp.where(places < fixed, places, passed)]].set(jnp.asarray(tallies, jnp.int32))

    tallies = jnp.where(number % 4 == 0, named(heavy_load, number // 4), named(usual, number - number // 4 - 1))
    mixed = jax.random.permutation(jax.random.fold_in(own, 3), amount)
    giver, sink = mixed[0:amount // 2 * 2:2], mixed[1:amount // 2 * 2:2]
    slack = jnp.minimum(tallies[giver] - 1, most - tallies[sink]) // 2
    slack = jnp.where((giver == order[0]) | (sink == order[0]) | (tallies[sink] == 0), 0, jnp.maximum(slack, 0))
    passed = jax.random.randint(jax.random.fold_in(own, 4), (amount // 2,), 0, 1 << 20) % (slack + 1)
    tallies = tallies.at[giver].add(-passed).at[sink].add(passed)
    items = jnp.searchsorted(jnp.cumsum(tallies), jnp.arange(rows * top), side="right").astype(jnp.int32)
    listing = items.reshape(top, rows).T
    listing = listing[jax.random.permutation(jax.random.fold_in(own, 1), rows)]
    rotation = jax.random.randint(jax.random.fold_in(own, 2), (rows, 1), 0, top)
    return jnp.take_along_axis(listing, (jnp.arange(top)[None, :] + rotation) % top, axis=1)


def load_shares(number_of, total, most, slope, full):
    weights = [(1 << 20) // math.isqrt(rank ** slope) + 1 for rank in range(1, number_of + 1)]
    largest = most if full else min(most, max(-(-total // number_of), total * weights[0] // sum(weights)))
    least = 1 if total - largest >= number_of - 1 else 0
    given, rest = [largest] + [least] * (number_of - 1), total - largest - least * (number_of - 1)
    while rest > 0:
        movable = [i for i in range(1, number_of) if given[i] < largest] or [i for i in range(1, number_of) if given[i] < most]
        mass, left = sum([weights[i] for i in movable]), rest
        for i in movable:
            more = min(most - given[i], max(1, left * weights[i] // mass), rest)
            given[i] = given[i] + more
            rest = rest - more
    return np.array(given)


def centred(stream_key, extent, scale, reach, shards=(), held_as=jnp.bfloat16):
    loudness = block_levels(stream_key, extent, shards, -0.22, 0.18) if shards else 1.0
    drawn = jax.random.normal(stream_key, extent, jnp.float32) * scale * loudness
    return jnp.minimum(jnp.maximum(drawn, -reach), reach).astype(held_as)


def setup_inputs(seed: int = 0) -> dict:
    key_list = jax.random.split(jax.random.key(seed), 17)
    queries = centred(key_list[0], (SEQ, MIX), 1.0, 6.0, ((0, 4), (1, 8)))
    cell_key_rows = centred(key_list[1], (SEQ, MIX), 1.0, 6.0, ((0, 4), (1, 8)))
    cell_value_rows = centred(key_list[2], (SEQ, MIX), 1.0, 6.0, ((0, 4), (1, 8)))
    output_gate_logits = centred(key_list[3], (SEQ, MIX), 1.0, 6.0, ((0, 4), (1, 8)))
    input_gate_logs = draw_input_gate_logs(jax.random.fold_in(key_list[16], 71), 0)
    forget_gate_logits = draw_forget_gate_logits(jax.random.fold_in(key_list[16], 71), 0)
    extra_log_forget = draw_extra_log_forget(jax.random.fold_in(key_list[16], 71), 0)
    head_norm_gain = jnp.clip(1.0 + 0.18 * jax.random.normal(key_list[7], (MIX,), jnp.float32), 0.1, 1.9)
    cell_output_matrix = centred(key_list[8], (MIX, D), MIX ** -0.5, 0.125, ((0, 8),))
    residual = centred(key_list[9], (SEQ, D), 1.0, 6.0, ((0, 4),))
    expert_norm_gain = jnp.clip(1.0 + 0.18 * jax.random.normal(key_list[10], (D,), jnp.float32), 0.1, 1.9)
    routes_keys = jax.random.split(jax.random.fold_in(key_list[11], 1), SEQ // TOK_DEV)
    routes_turns = jax.random.permutation(jax.random.fold_in(key_list[11], 3), SEQ // TOK_DEV)
    routes = jax.vmap(lambda own, number: assign_block(jax.random.fold_in(key_list[11], 2), own, number, TOK_DEV, EXPERTS, TOPK, CAP, 2))(routes_keys, routes_turns).reshape((SEQ, TOPK))
    token_expert_weights = jnp.clip(jnp.exp(math.log(1.0) - 1.609438 * jax.random.uniform(key_list[12], (SEQ, TOPK), jnp.float32) ** block_levels(key_list[12], (SEQ, TOPK), ((0, 4),), -0.2, 0.2)), 0.2, 1.0)
    expert_gate_matrix = centred(key_list[13], (EXPERTS, D, FF), D ** -0.5, 0.09375, ((0, 4), (2, 8)))
    expert_up_matrix = centred(key_list[14], (EXPERTS, D, FF), D ** -0.5, 0.09375, ((0, 4), (2, 8)))
    expert_down_matrix = centred(key_list[15], (EXPERTS, FF, D), FF ** -0.5, 0.125, ((0, 4), (1, 8)))
    return dict(queries=queries, cell_key_rows=cell_key_rows, cell_value_rows=cell_value_rows, output_gate_logits=output_gate_logits, input_gate_logs=input_gate_logs, forget_gate_logits=forget_gate_logits, extra_log_forget=extra_log_forget, head_norm_gain=head_norm_gain, cell_output_matrix=cell_output_matrix, residual=residual, expert_norm_gain=expert_norm_gain, routes=routes, token_expert_weights=token_expert_weights, expert_gate_matrix=expert_gate_matrix, expert_up_matrix=expert_up_matrix, expert_down_matrix=expert_down_matrix)


floor_neg = -1e+30
norm_eps = 1e-06
row_group = 128

def block_cells(query_f, key_f, value_f, input_f, forget_log_values, start_cell, start_stab):
    heads, length, width = query_f.shape
    count = length // BLOCK
    highest = lax.Precision.HIGHEST

    def split(array):
        return jnp.moveaxis(array.reshape((heads, count, BLOCK) + array.shape[2:]), 1, 0)
    causal = jnp.tril(jnp.ones((BLOCK, BLOCK), dtype=bool))

    def advance(carry, block):
        cell, stab = carry
        qblock, kblock, vblock, iblock, fblock = block
        cumul = jnp.cumsum(fblock, axis=-1)
        total = cumul[:, -1]
        log_inner = jnp.where(causal[None], cumul[:, :, None] - cumul[:, None, :] + iblock[:, None, :], floor_neg)
        carried = cumul + stab[:, None]
        stab_row = jnp.maximum(carried, lax.optimization_barrier(jnp.max(log_inner, axis=-1)))
        scores = jnp.einsum('hld,hsd->hls', qblock, kblock, precision=highest) * jnp.exp(log_inner - stab_row[..., None])
        numer = jnp.einsum('hls,hsd->hld', scores, vblock, precision=highest) + jnp.exp(carried - stab_row)[..., None] * jnp.einsum('hld,hde->hle', qblock, cell, precision=highest)
        log_write = total[:, None] - cumul + iblock
        stab_next = jnp.maximum(total + stab, lax.optimization_barrier(jnp.max(log_write, axis=-1)))
        weights = jnp.exp(log_write - stab_next[:, None])
        cell_next = jnp.exp(total + stab - stab_next)[:, None, None] * cell + jnp.einsum('hsd,hse->hde', kblock * weights[..., None], vblock, precision=highest)
        return ((cell_next, stab_next), (numer, stab_row))
    inputs = tuple((split(array) for array in (query_f, key_f, value_f, input_f, forget_log_values)))
    unused, (numer, stab_rows) = lax.scan(advance, (start_cell, start_stab), inputs)
    numer = jnp.moveaxis(numer, 0, 1).reshape(heads, length, width)
    stab_rows = jnp.moveaxis(stab_rows, 0, 1).reshape(heads, length)
    return (numer, stab_rows)

def rms_scale(rows, gain):
    values = rows.astype(jnp.float32)
    return (values * lax.rsqrt(lax.optimization_barrier(jnp.mean(values * values, axis=-1, keepdims=True)) + norm_eps) * gain).astype(jnp.bfloat16)

def expert_outputs(moe_in, routes, expert_gate_matrix, expert_up_matrix, expert_down_matrix):
    count = SEQ * TOPK
    expert = routes.reshape(-1).astype(jnp.int32)
    owner = jnp.arange(count, dtype=jnp.int32) // TOPK
    order = jnp.argsort(expert, stable=True).astype(jnp.int32)
    sorted_expert = expert[order]
    loads = lax.optimization_barrier(jnp.sum((expert[:, None] == jnp.arange(EXPERTS, dtype=jnp.int32)[None, :]).astype(jnp.int32), axis=0))
    starts = (jnp.cumsum(loads) - loads).astype(jnp.int32)
    padded = ((loads + row_group - 1) // row_group * row_group).astype(jnp.int32)
    ends = jnp.cumsum(padded).astype(jnp.int32)
    padded_starts = ends - padded
    dest = (padded_starts[sorted_expert] + jnp.arange(count, dtype=jnp.int32) - starts[sorted_expert]).astype(jnp.int32)
    room = (count + row_group - 1) // row_group * row_group + EXPERTS * row_group
    blocks = room // row_group
    row_owner = jnp.full((room,), SEQ, jnp.int32).at[dest].set(owner[order])
    block_first = jnp.arange(blocks, dtype=jnp.int32) * row_group
    block_expert = jnp.minimum(lax.optimization_barrier(jnp.sum((block_first[:, None] >= ends[None, :]).astype(jnp.int32), axis=1)), EXPERTS - 1).astype(jnp.int32)
    padded_in = jnp.concatenate([moe_in, jnp.zeros((1, D), moe_in.dtype)], axis=0)
    block_rows = padded_in[row_owner].reshape(blocks, row_group, D)
    width = FF // N_TP

    def one_block(args):
        rows, which = args
        gate = jnp.dot(rows, expert_gate_matrix[which], preferred_element_type=jnp.float32)
        upper = jnp.dot(rows, expert_up_matrix[which], preferred_element_type=jnp.float32)
        hidden = (jax.nn.silu(gate) * upper).astype(jnp.bfloat16)
        parts = jnp.einsum('rjf,jfd->rjd', hidden.reshape(row_group, N_TP, width).astype(jnp.float32), expert_down_matrix[which].reshape(N_TP, width, D).astype(jnp.float32))
        parts = lax.optimization_barrier(parts.astype(jnp.bfloat16)).astype(jnp.float32)
        return lax.optimization_barrier(jnp.sum(parts, axis=1)).astype(jnp.bfloat16)
    outputs = lax.map(one_block, (block_rows, block_expert)).reshape(room, D)
    place = jnp.zeros((count,), jnp.int32).at[order].set(dest)
    return outputs[place].reshape(SEQ, TOPK, D)

def reference(queries, cell_key_rows, cell_value_rows, output_gate_logits, input_gate_logs, forget_gate_logits, extra_log_forget, head_norm_gain, cell_output_matrix, residual, expert_norm_gain, routes, token_expert_weights, expert_gate_matrix, expert_up_matrix, expert_down_matrix):

    def heads_of(array):
        return jnp.transpose(array.astype(jnp.float32).reshape(SEQ, HEADS, HEAD_DIM), (1, 0, 2))
    query_f = heads_of(queries)
    key_f = heads_of(cell_key_rows) * HEAD_DIM ** (-0.5)
    value_f = heads_of(cell_value_rows)
    forget_log_values = jax.nn.log_sigmoid(forget_gate_logits) + extra_log_forget
    numer, stab_rows = block_cells(query_f, key_f, value_f, input_gate_logs, forget_log_values, jnp.zeros((HEADS, HEAD_DIM, HEAD_DIM), jnp.float32), jnp.zeros((HEADS,), jnp.float32))
    scaled = numer * lax.rsqrt(lax.optimization_barrier(jnp.mean(numer * numer, axis=2, keepdims=True)) + norm_eps) * head_norm_gain.reshape(HEADS, 1, HEAD_DIM)
    mixed = jnp.transpose(scaled, (1, 0, 2)).reshape(SEQ, MIX)
    cell_out = (jax.nn.sigmoid(output_gate_logits.astype(jnp.float32)) * mixed).astype(jnp.bfloat16)
    projected = jnp.dot(cell_out, cell_output_matrix, preferred_element_type=jnp.float32)
    after_mix = (residual.astype(jnp.float32) + projected).astype(jnp.bfloat16)
    moe_in = rms_scale(after_mix, expert_norm_gain)
    chosen = expert_outputs(moe_in, routes, expert_gate_matrix, expert_up_matrix, expert_down_matrix)
    moe = lax.optimization_barrier(jnp.sum(token_expert_weights[:, :, None] * chosen.astype(jnp.float32), axis=1))
    return (after_mix.astype(jnp.float32) + moe).astype(jnp.bfloat16)
```

```python
import functools

import jax
import jax.numpy as jnp
from jax import lax
from jax.experimental import pallas as pl
from jax.experimental.pallas import tpu as pltpu
from jax.sharding import Mesh, PartitionSpec as P

HEAD_DIM = 128
floor_neg = -1e30
norm_eps = 1e-06
HIGHEST = lax.Precision.HIGHEST
F32 = jnp.float32
BF16 = jnp.bfloat16


def swap_cores(x):
    return lax.ppermute(x, "core", ((0, 1), (1, 0)))


MESH = pl.DeviceIdType.MESH


def expert_cuts(width):
    tiles = width // 128
    late = max(2, round(tiles * 2 / 9))
    early = tiles - late
    a = (early + 1) // 2 * 128
    b = early * 128
    c = b + (late + 1) // 2 * 128
    return a, b, c


def slots(sizes):
    offsets, total = {}, 0
    for name, count in sizes:
        offsets[name] = total
        total += count
    return offsets, total


def expert_slots(nz):
    per_z = ("PZu", "PZd", "PX", "PY", "P3A", "P3B", "XA", "XB", "YA", "YB", "RX", "RY")
    per_z += ("SZu", "SZd")
    per_q = ("QZu", "QZd", "TZu", "TZd")
    single = ("QX", "QY", "Q3A", "Q3B", "TXA", "TXB", "TYA", "TYB", "TRX", "TRY")
    single += ("G", "U", "W")
    return slots(
        [(n, nz) for n in per_z] + [(n, 4 * nz) for n in per_q] + [(n, 1) for n in single]
    )


def expert_kernel(
    nz,
    after_ref,
    gain_ref,
    weight_ref,
    gate_hbm,
    up_hbm,
    down_hbm,
    out_ref,
    X,
    part,
    LX,
    LY,
    R,
    ZB,
    ZA,
    QB,
    QA,
    wg,
    wu,
    wd,
    act,
    send_sems,
    recv_sems,
    load_sems,
):
    T, width = after_ref.shape
    ca, cb, cc = expert_cuts(width)
    colA, colB, colP = pl.ds(0, ca), pl.ds(ca, cb - ca), pl.ds(0, cb)
    colQ, colQA, colQB = pl.ds(cb, width - cb), pl.ds(cb, cc - cb), pl.ds(cc, width - cc)
    subA, subB = pl.ds(0, cc - cb), pl.ds(cc - cb, width - cc)
    offsets, _ = expert_slots(nz)
    s, z, core = lax.axis_index("sp"), lax.axis_index("z"), lax.axis_index("core")
    to_x, to_y = (s ^ 1, z, core), (s ^ 2, z, core)
    to_up, to_down, to_peer = (s, z + 1, core), (s, z - 1, core), (s, z, 1 - core)
    has_up, has_down = z < nz - 1, z > 0
    always = None
    sent = []

    def when(cond, body):
        if cond is None:
            body()
        else:
            pl.when(cond)(body)

    def rows(index):
        return pl.ds(pl.multiple_of(index * T, 16), T)

    def copy(name, index, src, dst, to):
        at = offsets[name] + index
        return pltpu.make_async_remote_copy(
            src_ref=src,
            dst_ref=dst,
            send_sem=send_sems.at[at],
            recv_sem=recv_sems.at[at],
            device_id=to,
            device_id_type=MESH,
        )

    def send(cond, name, index, src, dst, to):
        when(cond, lambda: copy(name, index, src(), dst(), to).start())
        sent.append((cond, name, index, src, dst, to))

    def arrive(cond, name, index, dst):
        when(cond, lambda: copy(name, index, dst(), dst(), to_peer).wait_recv())

    loads = [
        pltpu.make_async_copy(src, dst.at[0], load_sems.at[i])
        for i, (src, dst) in enumerate(((gate_hbm, wg), (up_hbm, wu), (down_hbm, wd)))
    ]
    for load in loads:
        load.start()

    values = after_ref[...].astype(F32)
    scale = lax.rsqrt(jnp.mean(values * values, axis=-1, keepdims=True) + norm_eps)
    X[0, rows(z), :] = (values * scale * gain_ref[...]).astype(BF16)

    barrier = pltpu.get_barrier_semaphore()
    for cond, to in (
        (always, to_x),
        (always, to_y),
        (always, to_peer),
        (has_up, to_up),
        (has_down, to_down),
    ):
        when(
            cond,
            lambda to=to: pl.semaphore_signal(
                barrier, inc=1, device_id=to, device_id_type=MESH
            ),
        )
    pl.semaphore_wait(barrier, 3 + (z + nz - 1) // nz + (2 * (nz - 1) - z) // nz)

    def sides(d):
        return ((z >= d, z - d, "u"), (z + d < nz, z + d, "d"))

    def xblk(r, zs, cols):
        return lambda: X.at[r, rows(zs), cols]

    def z_p(way, zs, cond):
        go, to = (has_up, to_up) if way == "u" else (has_down, to_down)
        go = go if cond is None else cond & go
        send(go, "PZ" + way, zs, xblk(0, zs, colP), xblk(0, zs, colP), to)

    def z_q(way, r, zs, cond):
        go, to = (has_up, to_up) if way == "u" else (has_down, to_down)
        go = go if cond is None else cond & go
        send(go, "QZ" + way, r * nz + zs, xblk(r, zs, colQ), xblk(r, zs, colQ), to)

    def xy_p(cond, zs):
        send(cond, "PX", zs, xblk(0, zs, colP), xblk(1, zs, colP), to_x)
        send(cond, "PY", zs, xblk(0, zs, colP), xblk(2, zs, colP), to_y)

    send(always, "QX", 0, xblk(0, z, colQ), xblk(1, z, colQ), to_x)
    send(always, "QY", 0, xblk(0, z, colQ), xblk(2, z, colQ), to_y)
    z_p("u", z, always)
    z_p("d", z, always)
    xy_p(always, z)
    z_q("u", 0, z, always)
    z_q("d", 0, z, always)
    arrive(always, "QX", 0, xblk(1, z, colQ))
    send(always, "Q3A", 0, xblk(1, z, colQA), xblk(3, z, colQA), to_y)
    arrive(always, "QY", 0, xblk(2, z, colQ))
    send(always, "Q3B", 0, xblk(2, z, colQB), xblk(3, z, colQB), to_x)
    for load, name, buf in zip(loads, ("G", "U", "W"), (wg, wu, wd)):
        load.wait()
        send(always, name, 0, lambda buf=buf: buf.at[0], lambda buf=buf: buf.at[1], to_peer)

    for d in range(1, nz):
        for cond, zs, way in sides(d):
            arrive(cond, "PZ" + way, zs, xblk(0, zs, colP))
            z_p(way, zs, cond)
            xy_p(cond, zs)
        if d == 1:
            for r in (1, 2):
                z_q("u", r, z, always)
                z_q("d", r, z, always)
        if d == min(2, nz - 1):
            arrive(always, "Q3A", 0, xblk(3, z, colQA))
            arrive(always, "Q3B", 0, xblk(3, z, colQB))
            z_q("u", 3, z, always)
            z_q("d", 3, z, always)

    def diagonal(cond, zs):
        arrive(cond, "PX", zs, xblk(1, zs, colP))
        send(cond, "P3A", zs, xblk(1, zs, colA), xblk(3, zs, colA), to_y)
        arrive(cond, "PY", zs, xblk(2, zs, colP))
        send(cond, "P3B", zs, xblk(2, zs, colB), xblk(3, zs, colB), to_x)

    def q_forward(r, d):
        for cond, zs, way in sides(d):
            go = has_up if way == "u" else has_down
            arrive(cond & go, "QZ" + way, r * nz + zs, xblk(r, zs, colQ))
            z_q(way, r, zs, cond)

    def q_rest(r):
        for d in range(1, nz):
            for cond, zs, way in sides(d):
                stop = jnp.logical_not(has_up if way == "u" else has_down)
                arrive(cond & stop, "QZ" + way, r * nz + zs, xblk(r, zs, colQ))

    forwards = sorted(
        [(r, d) for r in range(4) for d in range(1, nz - 1)],
        key=lambda at: (at[0] + 2 * at[1], -at[1]),
    )
    share = len(forwards) / (nz - 1)
    diagonal(always, z)
    for d in range(1, nz):
        for r, far_d in forwards[round((d - 1) * share) : round(d * share)]:
            q_forward(r, far_d)
        for cond, zs, way in sides(d):
            diagonal(cond, zs)
    for name, buf in zip(("G", "U", "W"), (wg, wu, wd)):
        arrive(always, name, 0, lambda buf=buf: buf.at[1])

    step = min(1024, width)

    def compute(r):
        q_rest(r)
        if r == 3:
            for k in range(nz):
                arrive(always, "P3A", k, xblk(3, k, colA))
                arrive(always, "P3B", k, xblk(3, k, colB))

        @pl.loop(0, 2)
        def _(n):
            gate = jnp.dot(X[r], wg[n], preferred_element_type=F32)
            upper = jnp.dot(X[r], wu[n], preferred_element_type=F32)
            act[n] = (jax.nn.silu(gate) * upper).astype(BF16)

        @pl.loop(0, width // step)
        def _(n):
            cols = pl.ds(pl.multiple_of(n * step, step), step)
            total = jnp.dot(act[0], wd[0, :, cols], preferred_element_type=F32) + jnp.dot(
                act[1], wd[1, :, cols], preferred_element_type=F32
            )
            part[r, :, cols] = (total * weight_ref[r]).astype(BF16)

    def far(k):
        def one(a):
            low = (a - k - 1 + nz) // nz
            return low * (nz - 1 - k) + (1 - low) * (k - a)

        high = z // (nz // 2)
        return (1 - high) * one(nz - 1 - z) + high * (nz - 1 - one(z))

    order = [far(k) for k in range(nz)]

    def pblk(r, zd, cols):
        return lambda: part.at[r, rows(zd), cols]

    def lblk(buf, zd, cols):
        return lambda: buf.at[rows(zd), cols]

    def add(r, zd, cols, *others):
        total = part[r, rows(zd), cols].astype(F32)
        for buf in others:
            total = total + buf[rows(zd), cols].astype(F32)
        part[r, rows(zd), cols] = total.astype(BF16)

    def t_send(cond, r, zd, way):
        buf, to = (QB, to_up) if way == "u" else (QA, to_down)
        send(cond, "TZ" + way, r * nz + zd, pblk(r, zd, colQ), lambda: buf.at[r, rows(zd), :], to)

    def t_take(r, zd, way):
        buf = QB if way == "u" else QA
        at = buf.at[r, rows(zd), :]
        copy("TZ" + way, r * nz + zd, at, at, to_peer).wait_recv()
        part[r, rows(zd), colQ] = (
            part[r, rows(zd), colQ].astype(F32) + buf[r, rows(zd), :].astype(F32)
        ).astype(BF16)

    def t_hop(r, h):
        low, high = z == h, z == nz - 1 - h
        for zd in reversed(range(h + 1, nz)):
            if h:
                pl.when(low)(lambda zd=zd: t_take(r, zd, "u"))
            t_send(low, r, zd, "u")
        for zd in range(nz - 1 - h):
            if h:
                pl.when(high)(lambda zd=zd: t_take(r, zd, "d"))
            t_send(high, r, zd, "d")

    def t_own(r):
        pl.when(has_down)(lambda: t_take(r, z, "u"))
        pl.when(has_up)(lambda: t_take(r, z, "d"))

    def x_direct(k):
        zd = order[k]
        send(always, "XB", zd, pblk(1, zd, colB), lblk(LX, zd, colB), to_x)

    def y_direct(k):
        zd = order[k]
        send(always, "YA", zd, pblk(2, zd, colA), lblk(LY, zd, colA), to_y)

    def issue(k):
        zd = order[k]
        if k:
            x_direct(k)
            y_direct(k)
        arrive(always, "RY", zd, lblk(R, zd, colA))
        add(1, zd, colA, R)
        send(always, "XA", zd, pblk(1, zd, colA), lblk(LX, zd, colA), to_x)
        arrive(always, "RX", zd, lblk(R, zd, colB))
        add(2, zd, colB, R)
        send(always, "YB", zd, pblk(2, zd, colB), lblk(LY, zd, colB), to_y)

    def s_send(cond, zd, way):
        buf, to = (ZB, to_up) if way == "u" else (ZA, to_down)
        send(cond, "SZ" + way, zd, pblk(0, zd, colP), lblk(buf, zd, colP), to)

    def square(k):
        zd = order[k]
        arrive(always, "XB", zd, lblk(LX, zd, colB))
        arrive(always, "YA", zd, lblk(LY, zd, colA))
        arrive(always, "XA", zd, lblk(LX, zd, colA))
        arrive(always, "YB", zd, lblk(LY, zd, colB))
        add(0, zd, colP, LX, LY)
        s_send((zd > z) & jnp.logical_not(has_down), zd, "u")
        s_send((zd < z) & jnp.logical_not(has_up), zd, "d")

    def line(k):
        zd = order[k]
        up_in, down_in = (zd >= z) & has_down, (zd <= z) & has_up
        arrive(up_in, "SZu", zd, lblk(ZB, zd, colP))
        when(up_in, lambda: add(0, zd, colP, ZB))
        arrive(down_in, "SZd", zd, lblk(ZA, zd, colP))
        when(down_in, lambda: add(0, zd, colP, ZA))
        s_send((zd > z) & has_down, zd, "u")
        s_send((zd < z) & has_up, zd, "d")

    def q_direct():
        send(always, "TXB", 0, pblk(1, z, colQB), lblk(LX, z, colQB), to_x)
        send(always, "TYA", 0, pblk(2, z, colQA), lblk(LY, z, colQA), to_y)
        send(always, "TRY", 0, pblk(3, z, colQA), lblk(R, z, colQA), to_y)
        send(always, "TRX", 0, pblk(3, z, colQB), lblk(R, z, colQB), to_x)

    def q_relay():
        arrive(always, "TRY", 0, lblk(R, z, colQA))
        add(1, z, colQA, R)
        send(always, "TXA", 0, pblk(1, z, colQA), lblk(LX, z, colQA), to_x)
        arrive(always, "TRX", 0, lblk(R, z, colQB))
        add(2, z, colQB, R)
        send(always, "TYB", 0, pblk(2, z, colQB), lblk(LY, z, colQB), to_y)

    hops = [[(r - h, h) for h in range(nz - 1) if 0 <= r - h < 4] for r in range(4 + nz - 2)]
    for r in range(4):
        compute(r)
        if r == 1:
            x_direct(0)
        if r == 2:
            y_direct(0)
        if r == 3:
            for k in range(nz):
                zd = order[k]
                send(always, "RY", zd, pblk(3, zd, colA), lblk(R, zd, colA), to_y)
                send(always, "RX", zd, pblk(3, zd, colB), lblk(R, zd, colB), to_x)
        for group, h in hops[r]:
            t_hop(group, h)
    for k in range(nz - 1):
        issue(k)
        if 4 + k < len(hops):
            for group, h in hops[4 + k]:
                t_hop(group, h)
    for r in range(4):
        t_own(r)
    q_direct()
    issue(nz - 1)
    q_relay()
    for k in range(nz - 1):
        square(k)
        line(k)
    arrive(always, "TXB", 0, lblk(LX, z, colQB))
    arrive(always, "TYA", 0, lblk(LY, z, colQA))
    arrive(always, "TXA", 0, lblk(LX, z, colQA))
    arrive(always, "TYB", 0, lblk(LY, z, colQB))
    out_ref[:, colQ] = (
        after_ref[:, colQ].astype(F32)
        + part[0, rows(z), colQ].astype(F32)
        + LX[rows(z), colQ].astype(F32)
        + LY[rows(z), colQ].astype(F32)
    ).astype(BF16)
    square(nz - 1)
    line(nz - 1)
    out_ref[:, colP] = (
        after_ref[:, colP].astype(F32) + part[0, rows(z), colP].astype(F32)
    ).astype(BF16)
    for cond, name, index, src, dst, to in sent:
        when(
            cond,
            lambda name=name, index=index, src=src, dst=dst, to=to: copy(
                name, index, src(), dst(), to
            ).wait_send(),
        )


def expert_stage(after_mix, gain, weights, gate, up, down, nz):
    T, width = after_mix.shape
    hidden = gate.shape[1]
    rows = nz * T
    late = width - expert_cuts(width)[1]
    _, count = expert_slots(nz)
    vmem, hbm = pl.BlockSpec(memory_space=pltpu.VMEM), pl.BlockSpec(memory_space=pl.ANY)
    plane = pltpu.VMEM((rows, width), BF16)
    side = pltpu.VMEM((4, rows, late), BF16)
    return pl.pallas_call(
        functools.partial(expert_kernel, nz),
        out_shape=jax.ShapeDtypeStruct((T, width), BF16),
        in_specs=[vmem, vmem, vmem, hbm, hbm, hbm],
        out_specs=vmem,
        scratch_shapes=[
            pltpu.VMEM((4, rows, width), BF16),
            pltpu.VMEM((4, rows, width), BF16),
            plane,
            plane,
            plane,
            plane,
            plane,
            side,
            side,
            pltpu.VMEM((2, width, hidden), BF16),
            pltpu.VMEM((2, width, hidden), BF16),
            pltpu.VMEM((2, hidden, width), BF16),
            pltpu.VMEM((2, rows, hidden), BF16),
            pltpu.SemaphoreType.DMA((count,)),
            pltpu.SemaphoreType.DMA((count,)),
            pltpu.SemaphoreType.DMA((3,)),
        ],
        compiler_params=pltpu.CompilerParams(
            collective_id=1, has_side_effects=True, vmem_limit_bytes=56 * 2**20
        ),
        name="experts",
    )(after_mix, gain, weights, gate, up, down)


def local(
    queries,
    cell_key_rows,
    cell_value_rows,
    output_gate_logits,
    input_gate_logs,
    forget_gate_logits,
    extra_log_forget,
    head_norm_gain,
    cell_output_matrix,
    residual,
    expert_norm_gain,
    routes,
    token_expert_weights,
    expert_gate_matrix,
    expert_up_matrix,
    expert_down_matrix,
):
    length = queries.shape[0]
    heads = queries.shape[1] // HEAD_DIM
    sp_count = lax.axis_size("sp")
    z_count = lax.axis_size("z")
    sp_index = lax.axis_index("sp")
    z_index = lax.axis_index("z")
    core = lax.axis_index("core")
    tokens = length // (z_count * 2)
    width = residual.shape[1]

    gate_own, up_own, down_own = expert_gate_matrix[0], expert_up_matrix[0], expert_down_matrix[0]
    mix_peer = swap_cores(cell_output_matrix)

    forget_log = jax.nn.log_sigmoid(forget_gate_logits) + extra_log_forget
    running = jnp.cumsum(forget_log, axis=1)
    total = running[:, -1]
    log_write = input_gate_logs + total[:, None] - running
    stab_dev = jnp.max(log_write, axis=1)
    write = jnp.exp(log_write - stab_dev[:, None])

    def head(array, h):
        return array[:, h * HEAD_DIM : (h + 1) * HEAD_DIM]

    scale = HEAD_DIM ** (-0.5)
    cell_dev = [
        lax.dot_general(
            head(cell_key_rows, h).astype(F32) * (write[h] * scale)[:, None],
            head(cell_value_rows, h).astype(F32),
            (((0,), (0,)), ((), ())),
            precision=HIGHEST,
        )
        for h in range(heads)
    ]
    token_gates = jnp.sum(
        jnp.where(
            routes[None, :, :] == jnp.arange(sp_count, dtype=routes.dtype)[:, None, None],
            token_expert_weights[None],
            0.0,
        ),
        axis=2,
    )
    scalars = jnp.pad(jnp.concatenate([stab_dev, total])[None], ((0, 7), (0, HEAD_DIM - 2 * heads)))
    pack = jnp.concatenate(cell_dev + [scalars, token_gates.reshape(-1, HEAD_DIM)], axis=0)
    packs = lax.all_gather(pack, "sp")
    cells = packs[:, : heads * HEAD_DIM].reshape(sp_count, heads, HEAD_DIM, HEAD_DIM)
    stabs = packs[:, heads * HEAD_DIM, :heads]
    totals = packs[:, heads * HEAD_DIM, heads : 2 * heads]
    gates = packs[:, heads * HEAD_DIM + 8 :].reshape(sp_count, sp_count, length)
    gates = lax.dynamic_index_in_dim(gates, sp_index, 1, keepdims=False)

    order = jnp.arange(sp_count)
    between = (order[None, :] > order[:, None]) & (order[None, :] < sp_index)
    after = jnp.sum(jnp.where(between[:, :, None], totals[None], 0.0), axis=1)
    earlier = order < sp_index
    levels = jnp.where(earlier[:, None], stabs + after, floor_neg)
    before_total = jnp.sum(jnp.where(earlier[:, None], totals, 0.0), axis=0)
    start_stab = jnp.maximum(jnp.max(levels, axis=0), before_total)
    mixing = jnp.where(earlier[:, None], jnp.exp(levels - start_stab[None]), 0.0)
    start_cell = jnp.sum(mixing[:, :, None, None] * cells, axis=0)

    causal = jnp.tril(jnp.ones((length, length), dtype=bool))
    log_inner = jnp.where(
        causal[None],
        running[:, :, None] - running[:, None, :] + input_gate_logs[:, None, :],
        floor_neg,
    )
    inner_max = jnp.max(log_inner, axis=-1)
    carried = running + start_stab[:, None]
    stab_row = jnp.maximum(carried, inner_max)
    inner_scale = jnp.exp(inner_max - stab_row)
    carry_scale = jnp.exp(carried - stab_row)
    outs = []
    for h in range(heads):
        query = head(queries, h)
        products = lax.dot_general(
            query, head(cell_key_rows, h), (((1,), (1,)), ((), ())), preferred_element_type=F32
        )
        scores = products * (scale * jnp.exp(log_inner[h] - inner_max[h][:, None]))
        inner = jnp.dot(scores, head(cell_value_rows, h).astype(F32), precision=HIGHEST)
        carry = jnp.dot(query.astype(F32), start_cell[h], precision=HIGHEST)
        numer = inner_scale[h][:, None] * inner + carry_scale[h][:, None] * carry
        outs.append(
            numer
            * lax.rsqrt(jnp.mean(numer * numer, axis=1, keepdims=True) + norm_eps)
            * head(head_norm_gain[None], h)
        )
    cell_out = (
        jax.nn.sigmoid(output_gate_logits.astype(F32)) * jnp.concatenate(outs, axis=1)
    ).astype(BF16)

    rows = cell_out.reshape(z_count, 2, tokens, cell_out.shape[1])
    mine = lax.dynamic_index_in_dim(rows, core, 1, keepdims=False)
    theirs = swap_cores(lax.dynamic_index_in_dim(rows, 1 - core, 1, keepdims=False))
    mine = mine.reshape(z_count * tokens, -1)
    theirs = theirs.reshape(z_count * tokens, -1)
    mixed = jnp.dot(mine, cell_output_matrix, preferred_element_type=F32) + jnp.dot(
        theirs, mix_peer, preferred_element_type=F32
    )
    projected = lax.psum_scatter(mixed.astype(BF16), "z", scatter_dimension=0, tiled=True)

    start = (z_index * 2 + core) * tokens
    own_residual = lax.dynamic_slice_in_dim(residual, start, tokens, 0)
    after_mix = (own_residual.astype(F32) + projected.astype(F32)).astype(BF16)
    weight = lax.dynamic_index_in_dim(
        gates.reshape(sp_count, z_count, 2, tokens), core, 2, keepdims=False
    ).reshape(sp_count, z_count * tokens, 1)
    if sp_count == 4:
        weights = jnp.stack(
            [lax.dynamic_index_in_dim(weight, sp_index ^ r, 0, keepdims=False) for r in range(4)]
        )
        return expert_stage(
            after_mix, expert_norm_gain[None], weights, gate_own, up_own, down_own, z_count
        )

    gate_peer, up_peer, down_peer = swap_cores(gate_own), swap_cores(up_own), swap_cores(down_own)
    values = after_mix.astype(F32)
    moe_in = (
        values
        * lax.rsqrt(jnp.mean(values * values, axis=-1, keepdims=True) + norm_eps)
        * expert_norm_gain
    ).astype(BF16)
    half = width // 2
    cuts = (slice(0, half), slice(half, width))
    pieces = []
    for cut in cuts:
        line = lax.all_gather(moe_in[:, cut], "z", axis=0, tiled=True)
        pieces.append(lax.all_gather(line, "sp", axis=0, tiled=True))

    def project(matrix):
        return sum(
            jnp.dot(pieces[i], matrix[cut], preferred_element_type=F32)
            for i, cut in enumerate(cuts)
        )

    def hidden(gate_matrix, up_matrix):
        return (jax.nn.silu(project(gate_matrix)) * project(up_matrix)).astype(BF16)

    act = jnp.concatenate([hidden(gate_own, up_own), hidden(gate_peer, up_peer)], axis=1)
    down = jnp.concatenate([down_own, down_peer], axis=0)
    moe = []
    for cut in cuts:
        term = jnp.dot(act, down[:, cut], preferred_element_type=F32) * weight.reshape(-1, 1)
        summed = lax.psum_scatter(term.astype(BF16), "sp", scatter_dimension=0, tiled=True)
        moe.append(lax.psum_scatter(summed, "z", scatter_dimension=0, tiled=True))
    moe = jnp.concatenate(moe, axis=1)
    return (after_mix.astype(F32) + moe.astype(F32)).astype(BF16)


def solution(mesh):
    fine = Mesh(
        mesh.devices.reshape(mesh.shape["sp"], mesh.shape["tp"] // 2, 2), ("sp", "z", "core")
    )
    tp = ("z", "core")
    placed = (
        P("sp", tp),
        P("sp", tp),
        P("sp", tp),
        P("sp", tp),
        P(tp, "sp"),
        P(tp, "sp"),
        P(tp, "sp"),
        P(tp),
        P(tp, None),
        P("sp", None),
        P(),
        P("sp", None),
        P("sp", None),
        P("sp", None, tp),
        P("sp", None, tp),
        P("sp", tp, None),
    )
    return jax.shard_map(
        local, mesh=fine, in_specs=placed, out_specs=P(("sp", "z", "core"), None), check_vma=False
    )
```

```python
import functools

import jax
import jax.numpy as jnp
from jax import lax
from jax.experimental import pallas as pl
from jax.experimental.pallas import tpu as pltpu
from jax.sharding import Mesh, PartitionSpec as P

HEAD_DIM = 128
floor_neg = -1e30
norm_eps = 1e-06
HIGHEST = lax.Precision.HIGHEST
F32 = jnp.float32
BF16 = jnp.bfloat16


def swap_cores(x):
    return lax.ppermute(x, "core", ((0, 1), (1, 0)))


MESH = pl.DeviceIdType.MESH


def expert_cuts(width):
    tiles = width // 128
    late = max(2, round(tiles * 2 / 9))
    early = tiles - late
    a = (early + 1) // 2 * 128
    b = early * 128
    c = b + late // 2 * 128
    return a, b, c


def halves(x):
    high = x.astype(BF16)
    return high, (x - high.astype(F32)).astype(BF16)


def lanes(row):
    return jnp.transpose(jnp.broadcast_to(row, (HEAD_DIM, row.shape[1])))


FIRST = ("WZ", "WX", "WY", "W3A", "W3B", "WP", "SQ", "CE", "MT")
FIRST += ("CX", "CY", "CD", "SX", "SY", "SD", "RX1", "RY1", "RD1")


def semaphore_slots(nz):
    first = [(n, nz) for n in FIRST[:7]] + [("CE", 2 * nz + 2)]
    first += [(n, 1) for n in FIRST[8:]]
    sums = [(n, nz) for n in ("XA", "XB", "YA", "YB", "RX", "RY")]
    sums += [("SZ", nz + 1), ("TZ", 4 * nz + 4)]
    sums += [(n, 1) for n in ("TXA", "TXB", "TYA", "TYB", "TRX", "TRY")]
    gather = [("PZ", nz + 1), ("QZ", 4 * nz + 4)]
    gather += [(n, nz) for n in ("PX", "PY", "P3A", "P3B")]
    gather += [(n, 1) for n in ("QX", "QY", "Q3A", "Q3B", "TX", "TY", "TD", "G", "U", "W")]
    offsets = {}

    def place(kinds, at):
        for name, count in kinds:
            offsets[name] = at
            at += count
        return at

    return offsets, place(gather, max(place(first, 0), place(sums, 0)))


def layer_kernel(
    nz,
    q_hbm,
    k_hbm,
    v_hbm,
    og_hbm,
    ig_hbm,
    fg_hbm,
    ef_hbm,
    hg_hbm,
    gain_hbm,
    routes_hbm,
    choice_hbm,
    mix_hbm,
    res_hbm,
    gate_hbm,
    up_hbm,
    down_hbm,
    out_ref,
    q_ref,
    k_ref,
    v_ref,
    og_ref,
    ig_ref,
    fg_ref,
    ef_ref,
    hg_ref,
    gain_ref,
    routes_ref,
    choice_ref,
    after_ref,
    cells,
    marks,
    tgs,
    inner_ref,
    imax_ref,
    rcol_ref,
    cell_ref,
    ce,
    wcol_ref,
    weight_ref,
    wown,
    wz,
    res,
    squares,
    roots,
    X,
    part,
    LX,
    LY,
    R,
    ZB,
    ZA,
    QB,
    QA,
    wg,
    wu,
    wd,
    act,
    send_sems,
    recv_sems,
    load_sems,
):
    T, width = out_ref.shape
    rows_all, wide = after_ref.shape
    ga, gb, gc = expert_cuts(wide)
    colGA, colGB, colGP = pl.ds(0, ga), pl.ds(ga, gb - ga), pl.ds(0, gb)
    colGQ, colGQA, colGQB = pl.ds(gb, wide - gb), pl.ds(gb, gc - gb), pl.ds(gc, wide - gc)
    ca, cb, cc = expert_cuts(width)
    colA, colB, colP = pl.ds(0, ca), pl.ds(ca, cb - ca), pl.ds(0, cb)
    colQ, colQA, colQB = pl.ds(cb, width - cb), pl.ds(cb, cc - cb), pl.ds(cc, width - cc)
    subA, subB = pl.ds(0, cc - cb), pl.ds(cc - cb, width - cc)
    offsets, _ = semaphore_slots(nz)
    s, z, core = lax.axis_index("sp"), lax.axis_index("z"), lax.axis_index("core")
    to_x, to_y = (s ^ 1, z, core), (s ^ 2, z, core)
    to_up, to_down, to_peer = (s, z + 1, core), (s, z - 1, core), (s, z, 1 - core)
    to_diag = (s ^ 3, z, core)
    has_up, has_down = z < nz - 1, z > 0
    always = None
    sent = []

    def when(cond, body):
        if cond is None:
            body()
        else:
            pl.when(cond)(body)

    def rows(index):
        return pl.ds(pl.multiple_of(index * T, 16), T)

    def copy(name, index, src, dst, to, out=None):
        at = offsets[name] + index
        return pltpu.make_async_remote_copy(
            src_ref=src,
            dst_ref=dst,
            send_sem=send_sems.at[at if out is None else offsets[name] + out],
            recv_sem=recv_sems.at[at],
            device_id=to,
            device_id_type=MESH,
        )

    def send(cond, name, index, src, dst, to, out=None):
        when(cond, lambda: copy(name, index, src(), dst(), to, out).start())
        sent.append((cond, name, index, src, dst, to, out))

    def drain(entries):
        for entry in entries:
            cond, name, index, src, dst, to, out = entry
            when(
                cond,
                lambda name=name, index=index, src=src, dst=dst, to=to, out=out: copy(
                    name, index, src(), dst(), to, out
                ).wait_send(),
            )
        done = [id(entry) for entry in entries]
        sent[:] = [entry for entry in sent if id(entry) not in done]

    def arrive(cond, name, index, dst):
        when(cond, lambda: copy(name, index, dst(), dst(), to_peer).wait_recv())

    barrier = pltpu.get_barrier_semaphore()
    for cond, to in (
        (always, to_x),
        (always, to_y),
        (always, to_diag),
        (always, to_peer),
    ) + tuple((z != k, (s, k, core)) for k in range(nz)):
        when(
            cond,
            lambda to=to: pl.semaphore_signal(
                barrier, inc=1, device_id=to, device_id_type=MESH
            ),
        )
    reads = [
        pltpu.make_async_copy(src, dst, load_sems.at[4 + nz + i])
        for i, (src, dst) in enumerate(
            (
                (fg_hbm, fg_ref),
                (ef_hbm, ef_ref),
                (ig_hbm, ig_ref),
                (k_hbm, k_ref),
                (v_hbm, v_ref),
                (q_hbm, q_ref),
                (og_hbm, og_ref),
                (hg_hbm, hg_ref),
                (gain_hbm, gain_ref),
                (routes_hbm, routes_ref),
                (choice_hbm, choice_ref),
            )
        )
    ]
    for read in reads[:5]:
        read.start()
    zcols = pl.ds(pl.multiple_of(z * wide, 128), wide)
    load_mix = pltpu.make_async_copy(mix_hbm, wown, load_sems.at[3])
    load_res = [
        pltpu.make_async_copy(
            res_hbm.at[pl.ds(pl.multiple_of((k * 2 + core) * T, 16), T), zcols],
            res.at[k],
            load_sems.at[4 + k],
        )
        for k in range(nz)
    ]
    loads = [
        pltpu.make_async_copy(src, dst.at[0], load_sems.at[i])
        for i, (src, dst) in enumerate(((gate_hbm, wg), (up_hbm, wu), (down_hbm, wd)))
    ]
    load_mix.start()
    for load in reads[5:] + load_res + loads:
        load.start()

    length = q_ref.shape[0]
    heads = q_ref.shape[1] // HEAD_DIM
    scale = HEAD_DIM ** (-0.5)
    above = lax.broadcasted_iota(jnp.int32, (length, length), 0)
    along = lax.broadcasted_iota(jnp.int32, (length, length), 1)
    for read in reads[:3]:
        read.wait()
    forget_log = jax.nn.log_sigmoid(fg_ref[...]) + ef_ref[...]
    stacked = jnp.concatenate(
        [jnp.broadcast_to(forget_log[h : h + 1], (8, length)) for h in range(heads)], axis=0
    )
    running = jnp.dot(
        stacked,
        (above <= along).astype(F32),
        precision=HIGHEST,
        preferred_element_type=F32,
    )

    def head(ref, h):
        return ref[:, h * HEAD_DIM : (h + 1) * HEAD_DIM]

    runs = [running[8 * h : 8 * h + 1] for h in range(heads)]
    for read in reads[3:5]:
        read.wait()
    for h in range(heads):
        total = runs[h][:, length - 1 :]
        log_write = ig_ref[h : h + 1, :] + total - runs[h]
        stab = jnp.max(log_write, axis=1, keepdims=True)
        write = jnp.exp(log_write - stab) * scale
        high, low = halves(jnp.transpose(head(k_ref, h).astype(F32)) * write)
        value = head(v_ref, h)
        cell = jnp.dot(high, value, preferred_element_type=F32) + jnp.dot(
            low, value, preferred_element_type=F32
        )
        cells[0, h] = cell.astype(BF16)
        marks[0, h : h + 1, :] = jnp.broadcast_to(stab, (1, HEAD_DIM))
        marks[0, heads + h : heads + h + 1, :] = jnp.broadcast_to(total, (1, HEAD_DIM))

    pl.semaphore_wait(barrier, 4 + nz - 1)

    quarter = wown.shape[0] // 4
    part_rows = quarter // 2

    def wblk(k, q, first, count):
        at = pl.ds(pl.multiple_of(q * quarter + first, 16), count)
        return lambda: wz.at[k, core, at, :]

    load_mix.wait()
    at_s = pl.ds(pl.multiple_of(s * quarter, 16), quarter)
    for d in range(1, nz):
        for cond, k in ((z + d < nz, z + d), (z >= d, z - d)):
            send(
                cond,
                "WZ",
                z,
                lambda k=k: wown.at[at_s, pl.ds(pl.multiple_of(k * wide, 128), wide)],
                wblk(z, s, 0, quarter),
                (s, k, core),
                out=k,
            )

    square_of = (("X", 1, to_x), ("Y", 2, to_y), ("D", 3, to_diag))
    for way, r, to in square_of:
        send(always, "S" + way, 0, lambda: marks.at[0], lambda r=r: marks.at[r], to)
        send(always, "C" + way, 0, lambda: cells.at[0], lambda r=r: cells.at[r], to)
    send(always, "WP", z, lambda: wown.at[:, zcols], lambda: wz.at[z, core], to_peer)
    wz[z, core] = wown[:, zcols]

    for read in reads[5:]:
        read.wait()
    for h in range(heads):
        column = lanes(runs[h])
        ahead = ig_ref[h : h + 1, :] - runs[h]
        log_inner = jnp.where(
            above >= along,
            jnp.concatenate([column] * (length // HEAD_DIM), axis=1) + ahead,
            floor_neg,
        )
        inner_max = jnp.max(log_inner, axis=1, keepdims=True)
        products = lax.dot_general(
            head(q_ref, h),
            head(k_ref, h),
            (((1,), (1,)), ((), ())),
            preferred_element_type=F32,
        )
        high, low = halves(products * (scale * jnp.exp(log_inner - inner_max)))
        value = head(v_ref, h)
        inner_ref[h] = jnp.dot(high, value, preferred_element_type=F32) + jnp.dot(
            low, value, preferred_element_type=F32
        )
        imax_ref[h] = jnp.broadcast_to(inner_max, (length, HEAD_DIM))
        rcol_ref[h] = column

    def sides(d):
        return ((z >= d, z - d, "u"), (z + d < nz, z + d, "d"))

    def w_spread(d):
        for cond, k, _ in sides(d):
            arrive(cond, "WZ", k, wblk(k, s, 0, quarter))
            send(cond, "WX", k, wblk(k, s, 0, quarter), wblk(k, s, 0, quarter), to_x)
            send(cond, "WY", k, wblk(k, s, 0, quarter), wblk(k, s, 0, quarter), to_y)

    for e in range(4):
        given = jnp.where(routes_ref[...] == e, choice_ref[...], 0.0)
        tgs[0, e : e + 1, :] = jnp.sum(given, axis=0, keepdims=True)
    for way, r, to in square_of:
        send(always, "R" + way + "1", 0, lambda: tgs.at[0], lambda r=r: tgs.at[r], to)

    for way, r, to in square_of:
        arrive(always, "S" + way, 0, lambda r=r: marks.at[r])
        arrive(always, "C" + way, 0, lambda r=r: cells.at[r])
    for h in range(heads):
        stabs = [marks[s ^ g, h : h + 1, :] for g in range(4)]
        totals = [marks[s ^ g, heads + h : heads + h + 1, :] for g in range(4)]
        levels = []
        before = jnp.zeros((1, HEAD_DIM), F32)
        for g in reversed(range(4)):
            levels.insert(0, jnp.where(g < s, stabs[g] + before, floor_neg))
            before = before + jnp.where(g < s, totals[g], 0.0)
        start_stab = before
        for level in levels:
            start_stab = jnp.maximum(start_stab, level)
        start_cell = jnp.zeros((HEAD_DIM, HEAD_DIM), F32)
        for g in range(4):
            mixing = jnp.exp(levels[g] - start_stab)
            start_cell = start_cell + jnp.where(
                g < s, mixing * cells[s ^ g, h].astype(F32), 0.0
            )
        high, low = halves(start_cell)
        query = head(q_ref, h)
        carry = jnp.dot(query, high, preferred_element_type=F32) + jnp.dot(
            query, low, preferred_element_type=F32
        )
        carried = rcol_ref[h] + start_stab
        stab_row = jnp.maximum(carried, imax_ref[h])
        numer = (
            jnp.exp(imax_ref[h] - stab_row) * inner_ref[h] + jnp.exp(carried - stab_row) * carry
        )
        normed = (
            numer
            * lax.rsqrt(jnp.mean(numer * numer, axis=1, keepdims=True) + norm_eps)
            * hg_ref[:, h * HEAD_DIM : (h + 1) * HEAD_DIM]
        )
        mixed = (jax.nn.sigmoid(head(og_ref, h).astype(F32)) * normed).astype(BF16)
        for b in range(2 * nz):
            cell_ref[b // 2, b % 2, :, h * HEAD_DIM : (h + 1) * HEAD_DIM] = mixed[
                b * T : (b + 1) * T
            ]

    def ce_send(way, k, j, cond):
        go, to = (has_up, to_up) if way == "u" else (has_down, to_down)
        go = go if cond is None else cond & go
        block = lambda: ce.at[k, (core + j) % 2]
        out = 2 * nz + j if cond is None and way == "d" else None
        send(go, "CE", k * 2 + j, block, block, to, out=out)

    send(always, "MT", 0, lambda: cell_ref.at[:, 1 - core], lambda: ce.at[z, core], to_peer)
    ce[z, core] = cell_ref[:, core]
    ce_send("u", z, 0, always)
    ce_send("d", z, 0, always)
    arrive(always, "MT", 0, lambda: ce.at[z, 1 - core])
    ce_send("u", z, 1, always)
    ce_send("d", z, 1, always)
    for d in range(1, nz):
        w_spread(d)
    ends = jnp.logical_not(has_up & has_down)

    def w_relay(d, also):
        for cond, k, _ in sides(d):
            cond = cond & also
            arrive(cond, "WX", k, wblk(k, s ^ 1, 0, quarter))
            top = wblk(k, s ^ 1, 0, part_rows)
            send(cond, "W3A", k, top, top, to_y)
            arrive(cond, "WY", k, wblk(k, s ^ 2, 0, quarter))
            low = wblk(k, s ^ 2, part_rows, part_rows)
            send(cond, "W3B", k, low, low, to_x)

    for d in range(1, nz):
        if d > 1:
            w_relay(d, ends)
        for j in range(2):
            for cond, k, way in sides(d):
                arrive(cond, "CE", k * 2 + j, lambda k=k, j=j: ce.at[k, (core + j) % 2])
                ce_send(way, k, j, cond)
        if d > 1:
            w_relay(d, has_up & has_down)
        else:
            w_relay(d, z >= 0)
    for d in range(1, nz):
        for cond, k, _ in sides(d):
            arrive(cond, "W3A", k, wblk(k, s ^ 3, 0, part_rows))
            arrive(cond, "W3B", k, wblk(k, s ^ 3, part_rows, part_rows))
            whole = lambda k=k: wz.at[k, core]
            send(cond, "WP", k, whole, whole, to_peer)
    for load in load_res:
        load.wait()
    for k in range(nz):
        arrive(always, "WP", k, lambda k=k: wz.at[k, 1 - core])
    share = wz.shape[2]
    step = min(512, wide)

    @pl.loop(0, wide // step)
    def _(n):
        cols = pl.ds(pl.multiple_of(n * step, step), step)
        total = res[:, :, cols].reshape(rows_all, step).astype(F32)
        for k in range(nz):
            for c in range(2):
                total = total + jnp.dot(
                    ce[k, c].reshape(rows_all, share),
                    wz[k, c, :, cols],
                    preferred_element_type=F32,
                )
        after_ref[:, cols] = total.astype(BF16)

    values = after_ref[...].astype(F32)
    X[0, z] = (values * gain_ref[:, zcols]).astype(BF16)

    def row_sums():
        square = values * values
        room = squares.shape[2] - rows_all
        square = jnp.concatenate([square, jnp.zeros((room, wide), F32)], axis=0)
        ones = jnp.ones((8, wide), BF16)
        dims = (((1,), (1,)), ((), ()))
        return sum(
            lax.dot_general(ones, piece, dims, preferred_element_type=F32)
            for piece in halves(square)
        )

    def xblk(r, zs, cols):
        return lambda: X.at[r, zs, :, cols]

    def z_p(way, zs, cond):
        go, to = (has_up, to_up) if way == "u" else (has_down, to_down)
        go = go if cond is None else cond & go
        out = nz if cond is None and way == "d" else None
        send(go, "PZ", zs, xblk(0, zs, colGP), xblk(0, zs, colGP), to, out=out)

    def z_q(way, r, zs, cond):
        go, to = (has_up, to_up) if way == "u" else (has_down, to_down)
        go = go if cond is None else cond & go
        out = 4 * nz + r if cond is None and way == "d" else None
        send(go, "QZ", r * nz + zs, xblk(r, zs, colGQ), xblk(r, zs, colGQ), to, out=out)

    def xy_p(cond, zs):
        send(cond, "PX", zs, xblk(0, zs, colGP), xblk(1, zs, colGP), to_x)
        send(cond, "PY", zs, xblk(0, zs, colGP), xblk(2, zs, colGP), to_y)

    send(always, "QX", 0, xblk(0, z, colGQ), xblk(1, z, colGQ), to_x)
    send(always, "QY", 0, xblk(0, z, colGQ), xblk(2, z, colGQ), to_y)
    z_p("u", z, always)
    z_p("d", z, always)
    xy_p(always, z)
    z_q("u", 0, z, always)
    z_q("d", 0, z, always)
    for load, name, buf in zip(loads, ("G", "U", "W"), (wg, wu, wd)):
        load.wait()
        send(always, name, 0, lambda buf=buf: buf.at[0], lambda buf=buf: buf.at[1], to_peer)

    for way, r, to in square_of:
        arrive(always, "R" + way + "1", 0, lambda r=r: tgs.at[r])
    for r in range(4):
        column = lanes(tgs[r, pl.ds(s, 1), :])
        for b in range(2 * nz):
            wcol_ref[b] = column[b * T : (b + 1) * T]
        for b in range(nz):
            weight_ref[r, b * T : (b + 1) * T, :] = wcol_ref[2 * b + core]

    squares[z] = row_sums()
    for k in range(nz):
        send(
            z != k,
            "SQ",
            z,
            lambda: squares.at[z],
            lambda: squares.at[z],
            (s, k, core),
            out=k,
        )
    arrive(always, "QX", 0, xblk(1, z, colGQ))
    send(always, "Q3A", 0, xblk(1, z, colGQA), xblk(3, z, colGQA), to_y)
    arrive(always, "QY", 0, xblk(2, z, colGQ))
    send(always, "Q3B", 0, xblk(2, z, colGQB), xblk(3, z, colGQB), to_x)

    for d in range(1, nz):
        for cond, zs, way in sides(d):
            arrive(cond, "PZ", zs, xblk(0, zs, colGP))
            z_p(way, zs, cond)
            xy_p(cond, zs)
        if d == 1:
            z_q("u", 1, z, always)
            z_q("d", 1, z, always)
        if d == min(2, nz - 1):
            z_q("u", 2, z, always)
            z_q("d", 2, z, always)
            arrive(always, "Q3A", 0, xblk(3, z, colGQA))
            arrive(always, "Q3B", 0, xblk(3, z, colGQB))
            z_q("u", 3, z, always)
            z_q("d", 3, z, always)

    def diagonal(cond, zs):
        arrive(cond, "PX", zs, xblk(1, zs, colGP))
        send(cond, "P3A", zs, xblk(1, zs, colGA), xblk(3, zs, colGA), to_y)
        arrive(cond, "PY", zs, xblk(2, zs, colGP))
        send(cond, "P3B", zs, xblk(2, zs, colGB), xblk(3, zs, colGB), to_x)

    def q_forward(r, d):
        for cond, zs, way in sides(d):
            go = has_up if way == "u" else has_down
            arrive(cond & go, "QZ", r * nz + zs, xblk(r, zs, colGQ))
            z_q(way, r, zs, cond)

    def q_rest(r):
        for d in range(1, nz):
            for cond, zs, way in sides(d):
                stop = jnp.logical_not(has_up if way == "u" else has_down)
                arrive(cond & stop, "QZ", r * nz + zs, xblk(r, zs, colGQ))

    forwards = sorted(
        [(r, d) for r in range(4) for d in range(1, nz - 1)],
        key=lambda at: (at[0] + 2 * at[1], -at[1]),
    )
    share = len(forwards) / (nz - 1)
    diagonal(always, z)
    for k in range(nz):
        arrive(z != k, "SQ", k, lambda k=k: squares.at[k])
    mean = sum(squares[k] for k in range(nz)) / width
    roots[0] = lax.rsqrt(mean + norm_eps)
    for way, r, to in square_of:
        send(always, "T" + way, 0, lambda: roots.at[0], lambda r=r: roots.at[r], to)
    for d in range(1, nz):
        for r, far_d in forwards[round((d - 1) * share) : round(d * share)]:
            q_forward(r, far_d)
        for cond, zs, way in sides(d):
            diagonal(cond, zs)
    for name, buf in zip(("G", "U", "W"), (wg, wu, wd)):
        arrive(always, name, 0, lambda buf=buf: buf.at[1])

    def compute(r):
        q_rest(r)
        if r == 3:
            for k in range(nz):
                arrive(always, "P3A", k, xblk(3, k, colGA))
                arrive(always, "P3B", k, xblk(3, k, colGB))

        if r:
            way = ("X", "Y", "D")[r - 1]
            arrive(always, "T" + way, 0, lambda: roots.at[r])
        root = lanes(roots[r][:1])[:rows_all, :1]

        @pl.loop(0, 2)
        def _(n):
            def project(matrix):
                return root * sum(
                    jnp.dot(
                        X[r, k],
                        matrix[n, k * wide : (k + 1) * wide, :],
                        preferred_element_type=F32,
                    )
                    for k in range(nz)
                )

            act[n] = (jax.nn.silu(project(wg)) * project(wu)).astype(BF16)

        @pl.loop(0, nz)
        def _(n):
            cols = pl.ds(pl.multiple_of(n * wide, wide), wide)
            total = jnp.dot(act[0], wd[0, :, cols], preferred_element_type=F32) + jnp.dot(
                act[1], wd[1, :, cols], preferred_element_type=F32
            )
            total = total * weight_ref[r][:, :1]
            if r == 0:
                total = total + jnp.where(n == z, after_ref[...].astype(F32), 0.0)
            part[r, :, cols] = total.astype(BF16)

    def far(k):
        def one(a):
            low = (a - k - 1 + nz) // nz
            return low * (nz - 1 - k) + (1 - low) * (k - a)

        high = z // (nz // 2)
        return (1 - high) * one(nz - 1 - z) + high * (nz - 1 - one(z))

    order = [far(k) for k in range(nz)]

    def pblk(r, zd, cols):
        return lambda: part.at[r, rows(zd), cols]

    def lblk(buf, zd, cols):
        return lambda: buf.at[rows(zd), cols]

    def add(r, zd, cols, *others):
        total = part[r, rows(zd), cols].astype(F32)
        for buf in others:
            total = total + buf[rows(zd), cols].astype(F32)
        part[r, rows(zd), cols] = total.astype(BF16)

    def t_send(cond, r, zd, way, last):
        buf, to = (QB, to_up) if way == "u" else (QA, to_down)
        at = 4 * nz + r if last and way == "d" else r * nz + zd
        send(cond, "TZ", at, pblk(r, zd, colQ), lambda: buf.at[r, rows(zd), :], to)

    def t_take(r, zd, way, last=False):
        buf = QB if way == "u" else QA
        ref = buf.at[r, rows(zd), :]
        at = 4 * nz + r if last and way == "d" else r * nz + zd
        copy("TZ", at, ref, ref, to_peer).wait_recv()
        part[r, rows(zd), colQ] = (
            part[r, rows(zd), colQ].astype(F32) + buf[r, rows(zd), :].astype(F32)
        ).astype(BF16)

    def t_hop(r, h):
        low, high = z == h, z == nz - 1 - h
        for zd in reversed(range(h + 1, nz)):
            if h:
                pl.when(low)(lambda zd=zd: t_take(r, zd, "u"))
            t_send(low, r, zd, "u", zd == h + 1)
        for zd in range(nz - 1 - h):
            if h:
                pl.when(high)(lambda zd=zd: t_take(r, zd, "d"))
            t_send(high, r, zd, "d", zd == nz - 2 - h)

    def t_own(r):
        pl.when(has_down)(lambda: t_take(r, z, "u", True))
        pl.when(has_up)(lambda: t_take(r, z, "d", True))

    def x_direct(k):
        zd = order[k]
        send(always, "XB", zd, pblk(1, zd, colB), lblk(LX, zd, colB), to_x)

    def y_direct(k):
        zd = order[k]
        send(always, "YA", zd, pblk(2, zd, colA), lblk(LY, zd, colA), to_y)

    def issue(k):
        zd = order[k]
        if k:
            x_direct(k)
            y_direct(k)
        arrive(always, "RY", zd, lblk(R, zd, colA))
        add(1, zd, colA, R)
        send(always, "XA", zd, pblk(1, zd, colA), lblk(LX, zd, colA), to_x)
        arrive(always, "RX", zd, lblk(R, zd, colB))
        add(2, zd, colB, R)
        send(always, "YB", zd, pblk(2, zd, colB), lblk(LY, zd, colB), to_y)

    def down_slot(zd, steps):
        last = 1 - (steps + nz - 1) // nz
        return zd + (nz - zd) * last

    def s_send(cond, zd, way):
        buf, to = (ZB, to_up) if way == "u" else (ZA, to_down)
        at = zd if way == "u" else down_slot(zd, z - 1 - zd)
        send(cond, "SZ", at, pblk(0, zd, colP), lblk(buf, zd, colP), to)

    def square(k):
        zd = order[k]
        arrive(always, "XB", zd, lblk(LX, zd, colB))
        arrive(always, "YA", zd, lblk(LY, zd, colA))
        arrive(always, "XA", zd, lblk(LX, zd, colA))
        arrive(always, "YB", zd, lblk(LY, zd, colB))
        add(0, zd, colP, LX, LY)
        s_send((zd > z) & jnp.logical_not(has_down), zd, "u")
        s_send((zd < z) & jnp.logical_not(has_up), zd, "d")

    def line(k):
        zd = order[k]
        up_in, down_in = (zd >= z) & has_down, (zd <= z) & has_up
        arrive(up_in, "SZ", zd, lblk(ZB, zd, colP))
        when(up_in, lambda: add(0, zd, colP, ZB))
        arrive(down_in, "SZ", down_slot(zd, z - zd), lblk(ZA, zd, colP))
        when(down_in, lambda: add(0, zd, colP, ZA))
        s_send((zd > z) & has_down, zd, "u")
        s_send((zd < z) & has_up, zd, "d")

    def q_direct():
        send(always, "TXB", 0, pblk(1, z, colQB), lblk(LX, z, colQB), to_x)
        send(always, "TYA", 0, pblk(2, z, colQA), lblk(LY, z, colQA), to_y)
        send(always, "TRY", 0, pblk(3, z, colQA), lblk(R, z, colQA), to_y)
        send(always, "TRX", 0, pblk(3, z, colQB), lblk(R, z, colQB), to_x)

    def q_relay():
        arrive(always, "TRY", 0, lblk(R, z, colQA))
        add(1, z, colQA, R)
        send(always, "TXA", 0, pblk(1, z, colQA), lblk(LX, z, colQA), to_x)
        arrive(always, "TRX", 0, lblk(R, z, colQB))
        add(2, z, colQB, R)
        send(always, "TYB", 0, pblk(2, z, colQB), lblk(LY, z, colQB), to_y)

    hops = [[(r - h, h) for h in range(nz - 1) if 0 <= r - h < 4] for r in range(4 + nz - 2)]
    drain([entry for entry in sent if entry[1] in FIRST])
    for r in range(4):
        compute(r)
        if r == 1:
            x_direct(0)
        if r == 2:
            y_direct(0)
        if r == 3:
            for k in range(nz):
                zd = order[k]
                send(always, "RY", zd, pblk(3, zd, colA), lblk(R, zd, colA), to_y)
                send(always, "RX", zd, pblk(3, zd, colB), lblk(R, zd, colB), to_x)
        for group, h in hops[r]:
            t_hop(group, h)
    early = list(sent)
    for k in range(nz - 1):
        issue(k)
        if 4 + k < len(hops):
            for group, h in hops[4 + k]:
                t_hop(group, h)
    for r in range(4):
        t_own(r)
    q_direct()
    issue(nz - 1)
    square(0)
    for k in range(1, nz - 1):
        square(k)
        line(k - 1)
    q_relay()
    line(nz - 2)
    drain(early)
    arrive(always, "TXB", 0, lblk(LX, z, colQB))
    arrive(always, "TYA", 0, lblk(LY, z, colQA))
    arrive(always, "TXA", 0, lblk(LX, z, colQA))
    arrive(always, "TYB", 0, lblk(LY, z, colQB))
    out_ref[:, colQ] = (
        part[0, rows(z), colQ].astype(F32)
        + LX[rows(z), colQ].astype(F32)
        + LY[rows(z), colQ].astype(F32)
    ).astype(BF16)
    square(nz - 1)
    line(nz - 1)
    out_ref[:, colP] = part[0, rows(z), colP]
    drain(list(sent))


def whole_layer(operands, tokens, nz):
    width = operands[11].shape[1]
    length, share = operands[0].shape
    heads = share // HEAD_DIM
    hidden = operands[13].shape[1]
    picks = operands[9].shape[0]
    rows = nz * tokens
    late = width - expert_cuts(width)[1]
    wide = width // nz
    room = (rows + HEAD_DIM - 1) // HEAD_DIM * HEAD_DIM
    _, count = semaphore_slots(nz)
    vmem, hbm = pl.BlockSpec(memory_space=pltpu.VMEM), pl.BlockSpec(memory_space=pltpu.HBM)
    plane = pltpu.VMEM((rows, width), BF16)
    side = pltpu.VMEM((4, rows, late), BF16)
    local_head = pltpu.VMEM((heads, length, HEAD_DIM), F32)
    return pl.pallas_call(
        functools.partial(layer_kernel, nz),
        out_shape=jax.ShapeDtypeStruct((tokens, width), BF16),
        in_specs=[hbm] * len(operands),
        out_specs=vmem,
        scratch_shapes=[
            *[pltpu.VMEM((length, share), BF16)] * 4,
            *[pltpu.VMEM((heads, length), F32)] * 3,
            pltpu.VMEM((1, share), F32),
            pltpu.VMEM((1, width), F32),
            pltpu.VMEM((picks, length), jnp.int32),
            pltpu.VMEM((picks, length), F32),
            pltpu.VMEM((rows, wide), BF16),
            pltpu.VMEM((4, heads, HEAD_DIM, HEAD_DIM), BF16),
            pltpu.VMEM((4, 8, HEAD_DIM), F32),
            pltpu.VMEM((4, 8, length), F32),
            local_head,
            local_head,
            local_head,
            pltpu.VMEM((nz, 2, tokens, share), BF16),
            pltpu.VMEM((nz, 2, nz, tokens, share), BF16),
            pltpu.VMEM((2 * nz, tokens, HEAD_DIM), F32),
            pltpu.VMEM((4, rows, HEAD_DIM), F32),
            pltpu.VMEM((share, width), BF16),
            pltpu.VMEM((nz, 2, share, wide), BF16),
            pltpu.VMEM((nz, tokens, wide), BF16),
            pltpu.VMEM((nz, 8, room), F32),
            pltpu.VMEM((4, 8, room), F32),
            pltpu.VMEM((4, nz, rows, wide), BF16),
            pltpu.VMEM((4, rows, width), BF16),
            plane,
            plane,
            plane,
            plane,
            plane,
            side,
            side,
            pltpu.VMEM((2, width, hidden), BF16),
            pltpu.VMEM((2, width, hidden), BF16),
            pltpu.VMEM((2, hidden, width), BF16),
            pltpu.VMEM((2, rows, hidden), BF16),
            pltpu.SemaphoreType.DMA((count,)),
            pltpu.SemaphoreType.DMA((count,)),
            pltpu.SemaphoreType.DMA((15 + nz,)),
        ],
        compiler_params=pltpu.CompilerParams(
            collective_id=1, has_side_effects=True, vmem_limit_bytes=63 * 2**20
        ),
        name="layer",
    )(*operands)


def local(
    queries,
    cell_key_rows,
    cell_value_rows,
    output_gate_logits,
    input_gate_logs,
    forget_gate_logits,
    extra_log_forget,
    head_norm_gain,
    cell_output_matrix,
    residual,
    expert_norm_gain,
    routes,
    token_expert_weights,
    expert_gate_matrix,
    expert_up_matrix,
    expert_down_matrix,
):
    length = queries.shape[0]
    heads = queries.shape[1] // HEAD_DIM
    sp_count = lax.axis_size("sp")
    z_count = lax.axis_size("z")
    sp_index = lax.axis_index("sp")
    z_index = lax.axis_index("z")
    core = lax.axis_index("core")
    tokens = length // (z_count * 2)
    width = residual.shape[1]

    gate_own, up_own, down_own = expert_gate_matrix[0], expert_up_matrix[0], expert_down_matrix[0]
    if sp_count == 4:
        operands = (
            queries,
            cell_key_rows,
            cell_value_rows,
            output_gate_logits,
            input_gate_logs,
            forget_gate_logits,
            extra_log_forget,
            head_norm_gain[None],
            expert_norm_gain[None],
            routes.T,
            token_expert_weights.T,
            cell_output_matrix,
            residual,
            gate_own,
            up_own,
            down_own,
        )
        return whole_layer(operands, tokens, z_count)

    token_gates = jnp.sum(
        jnp.where(
            routes[None, :, :] == jnp.arange(sp_count, dtype=routes.dtype)[:, None, None],
            token_expert_weights[None],
            0.0,
        ),
        axis=2,
    )
    mix_peer = swap_cores(cell_output_matrix)

    forget_log = jax.nn.log_sigmoid(forget_gate_logits) + extra_log_forget
    running = jnp.cumsum(forget_log, axis=1)
    total = running[:, -1]
    log_write = input_gate_logs + total[:, None] - running
    stab_dev = jnp.max(log_write, axis=1)
    write = jnp.exp(log_write - stab_dev[:, None])

    def head(array, h):
        return array[:, h * HEAD_DIM : (h + 1) * HEAD_DIM]

    scale = HEAD_DIM ** (-0.5)
    cell_dev = [
        lax.dot_general(
            head(cell_key_rows, h).astype(F32) * (write[h] * scale)[:, None],
            head(cell_value_rows, h).astype(F32),
            (((0,), (0,)), ((), ())),
            precision=HIGHEST,
        )
        for h in range(heads)
    ]
    scalars = jnp.pad(jnp.concatenate([stab_dev, total])[None], ((0, 7), (0, HEAD_DIM - 2 * heads)))
    pack = jnp.concatenate(cell_dev + [scalars, token_gates.reshape(-1, HEAD_DIM)], axis=0)
    packs = lax.all_gather(pack, "sp")
    cells = packs[:, : heads * HEAD_DIM].reshape(sp_count, heads, HEAD_DIM, HEAD_DIM)
    stabs = packs[:, heads * HEAD_DIM, :heads]
    totals = packs[:, heads * HEAD_DIM, heads : 2 * heads]
    gates = packs[:, heads * HEAD_DIM + 8 :].reshape(sp_count, sp_count, length)
    gates = lax.dynamic_index_in_dim(gates, sp_index, 1, keepdims=False)

    order = jnp.arange(sp_count)
    between = (order[None, :] > order[:, None]) & (order[None, :] < sp_index)
    after = jnp.sum(jnp.where(between[:, :, None], totals[None], 0.0), axis=1)
    earlier = order < sp_index
    levels = jnp.where(earlier[:, None], stabs + after, floor_neg)
    before_total = jnp.sum(jnp.where(earlier[:, None], totals, 0.0), axis=0)
    start_stab = jnp.maximum(jnp.max(levels, axis=0), before_total)
    mixing = jnp.where(earlier[:, None], jnp.exp(levels - start_stab[None]), 0.0)
    start_cell = jnp.sum(mixing[:, :, None, None] * cells, axis=0)

    causal = jnp.tril(jnp.ones((length, length), dtype=bool))
    log_inner = jnp.where(
        causal[None],
        running[:, :, None] - running[:, None, :] + input_gate_logs[:, None, :],
        floor_neg,
    )
    inner_max = jnp.max(log_inner, axis=-1)
    carried = running + start_stab[:, None]
    stab_row = jnp.maximum(carried, inner_max)
    inner_scale = jnp.exp(inner_max - stab_row)
    carry_scale = jnp.exp(carried - stab_row)
    outs = []
    for h in range(heads):
        query = head(queries, h)
        products = lax.dot_general(
            query, head(cell_key_rows, h), (((1,), (1,)), ((), ())), preferred_element_type=F32
        )
        scores = products * (scale * jnp.exp(log_inner[h] - inner_max[h][:, None]))
        inner = jnp.dot(scores, head(cell_value_rows, h).astype(F32), precision=HIGHEST)
        carry = jnp.dot(query.astype(F32), start_cell[h], precision=HIGHEST)
        numer = inner_scale[h][:, None] * inner + carry_scale[h][:, None] * carry
        outs.append(
            numer
            * lax.rsqrt(jnp.mean(numer * numer, axis=1, keepdims=True) + norm_eps)
            * head(head_norm_gain[None], h)
        )
    cell_out = (
        jax.nn.sigmoid(output_gate_logits.astype(F32)) * jnp.concatenate(outs, axis=1)
    ).astype(BF16)

    rows = cell_out.reshape(z_count, 2, tokens, cell_out.shape[1])
    mine = lax.dynamic_index_in_dim(rows, core, 1, keepdims=False)
    theirs = swap_cores(lax.dynamic_index_in_dim(rows, 1 - core, 1, keepdims=False))
    mine = mine.reshape(z_count * tokens, -1)
    theirs = theirs.reshape(z_count * tokens, -1)
    mixed = jnp.dot(mine, cell_output_matrix, preferred_element_type=F32) + jnp.dot(
        theirs, mix_peer, preferred_element_type=F32
    )
    projected = lax.psum_scatter(mixed.astype(BF16), "z", scatter_dimension=0, tiled=True)

    start = (z_index * 2 + core) * tokens
    own_residual = lax.dynamic_slice_in_dim(residual, start, tokens, 0)
    after_mix = (own_residual.astype(F32) + projected.astype(F32)).astype(BF16)
    weight = lax.dynamic_index_in_dim(
        gates.reshape(sp_count, z_count, 2, tokens), core, 2, keepdims=False
    ).reshape(sp_count, z_count * tokens, 1)
    gate_peer, up_peer, down_peer = swap_cores(gate_own), swap_cores(up_own), swap_cores(down_own)
    values = after_mix.astype(F32)
    moe_in = (
        values
        * lax.rsqrt(jnp.mean(values * values, axis=-1, keepdims=True) + norm_eps)
        * expert_norm_gain
    ).astype(BF16)
    half = width // 2
    cuts = (slice(0, half), slice(half, width))
    pieces = []
    for cut in cuts:
        line = lax.all_gather(moe_in[:, cut], "z", axis=0, tiled=True)
        pieces.append(lax.all_gather(line, "sp", axis=0, tiled=True))

    def project(matrix):
        return sum(
            jnp.dot(pieces[i], matrix[cut], preferred_element_type=F32)
            for i, cut in enumerate(cuts)
        )

    def hidden(gate_matrix, up_matrix):
        return (jax.nn.silu(project(gate_matrix)) * project(up_matrix)).astype(BF16)

    act = jnp.concatenate([hidden(gate_own, up_own), hidden(gate_peer, up_peer)], axis=1)
    down = jnp.concatenate([down_own, down_peer], axis=0)
    moe = []
    for cut in cuts:
        term = jnp.dot(act, down[:, cut], preferred_element_type=F32) * weight.reshape(-1, 1)
        summed = lax.psum_scatter(term.astype(BF16), "sp", scatter_dimension=0, tiled=True)
        moe.append(lax.psum_scatter(summed, "z", scatter_dimension=0, tiled=True))
    moe = jnp.concatenate(moe, axis=1)
    return (after_mix.astype(F32) + moe.astype(F32)).astype(BF16)


def solution(mesh):
    fine = Mesh(
        mesh.devices.reshape(mesh.shape["sp"], mesh.shape["tp"] // 2, 2), ("sp", "z", "core")
    )
    tp = ("z", "core")
    placed = (
        P("sp", tp),
        P("sp", tp),
        P("sp", tp),
        P("sp", tp),
        P(tp, "sp"),
        P(tp, "sp"),
        P(tp, "sp"),
        P(tp),
        P(tp, None),
        P("sp", None),
        P(),
        P("sp", None),
        P("sp", None),
        P("sp", None, tp),
        P("sp", None, tp),
        P("sp", tp, None),
    )
    return jax.shard_map(
        local, mesh=fine, in_specs=placed, out_specs=P(("sp", "z", "core"), None), check_vma=False
    )
```

```python
import functools

import jax
import jax.numpy as jnp
from jax import lax
from jax.experimental import pallas as pl
from jax.experimental.pallas import tpu as pltpu
from jax.sharding import Mesh, PartitionSpec as P

HEAD_DIM = 128
floor_neg = -1e30
norm_eps = 1e-06
HIGHEST = lax.Precision.HIGHEST
F32 = jnp.float32
BF16 = jnp.bfloat16


def swap_cores(x):
    return lax.ppermute(x, "core", ((0, 1), (1, 0)))


MESH = pl.DeviceIdType.MESH


def expert_cuts(width):
    tiles = width // 128
    late = round(tiles * 9 / 32)
    early = tiles - late
    a = (early + 1) // 2 * 128
    b = early * 128
    c = b + late // 2 * 128
    return a, b, c


def halves(x):
    high = x.astype(BF16)
    return high, (x - high.astype(F32)).astype(BF16)


def lanes(row):
    return jnp.transpose(jnp.broadcast_to(row, (HEAD_DIM, row.shape[1])))


FIRST = ("WZ", "WX", "WY", "W3A", "W3B", "WP", "SQ", "CE", "MT")
FIRST += ("CX", "CY", "CD", "SX", "SY", "SD", "RX1", "RY1", "RD1")


def semaphore_slots(nz):
    first = [(n, nz) for n in FIRST[:7]] + [("CE", 2 * nz + 2)]
    first += [(n, 1) for n in FIRST[8:]]
    sums = [(n, nz) for n in ("XA", "XB", "YA", "YB", "RX", "RY")]
    sums += [("SZ", nz + 1), ("TZ", 4 * nz + 4)]
    sums += [(n, 1) for n in ("TXA", "TXB", "TYA", "TYB", "TRX", "TRY")]
    gather = [("PZ", nz + 1), ("QZ", 4 * nz + 4)]
    gather += [(n, nz) for n in ("PX", "PY", "P3A", "P3B")]
    gather += [(n, 1) for n in ("QX", "QY", "Q3A", "TX", "TY", "TD", "G", "U", "W")]
    offsets = {}

    def place(kinds, at):
        for name, count in kinds:
            offsets[name] = at
            at += count
        return at

    return offsets, place(gather, max(place(first, 0), place(sums, 0)))


def layer_kernel(
    nz,
    q_hbm,
    k_hbm,
    v_hbm,
    og_hbm,
    ig_hbm,
    fg_hbm,
    ef_hbm,
    hg_hbm,
    gain_hbm,
    routes_hbm,
    choice_hbm,
    mix_hbm,
    res_hbm,
    gate_hbm,
    up_hbm,
    down_hbm,
    out_ref,
    q_ref,
    k_ref,
    v_ref,
    og_ref,
    ig_ref,
    fg_ref,
    ef_ref,
    hg_ref,
    gain_ref,
    routes_ref,
    choice_ref,
    after_ref,
    cells,
    marks,
    tgs,
    inner_ref,
    imax_ref,
    rcol_ref,
    cell_ref,
    ce,
    wcol_ref,
    weight_ref,
    wown,
    wz,
    res,
    squares,
    roots,
    X,
    part,
    LX,
    LY,
    R,
    ZB,
    ZA,
    QB,
    QA,
    wg,
    wu,
    wd,
    act,
    send_sems,
    recv_sems,
    load_sems,
):
    T, width = out_ref.shape
    rows_all, wide = after_ref.shape
    gb = wide - max(1, wide // 1024) * 128
    colGP, colGQ = pl.ds(0, gb), pl.ds(gb, wide - gb)

    def diag_cols(odd):
        cut = (gb // 128 + 1 - odd) // 2 * 128
        return pl.ds(0, cut), pl.ds(cut, gb - cut)

    ca, cb, cc = expert_cuts(width)
    colA, colB, colP = pl.ds(0, ca), pl.ds(ca, cb - ca), pl.ds(0, cb)
    colQ, colQA, colQB = pl.ds(cb, width - cb), pl.ds(cb, cc - cb), pl.ds(cc, width - cc)
    subA, subB = pl.ds(0, cc - cb), pl.ds(cc - cb, width - cc)
    offsets, _ = semaphore_slots(nz)
    s, z, core = lax.axis_index("sp"), lax.axis_index("z"), lax.axis_index("core")
    to_x, to_y = (s ^ 1, z, core), (s ^ 2, z, core)
    to_up, to_down, to_peer = (s, z + 1, core), (s, z - 1, core), (s, z, 1 - core)
    to_diag = (s ^ 3, z, core)
    has_up, has_down = z < nz - 1, z > 0
    always = None
    sent = []

    def when(cond, body):
        if cond is None:
            body()
        else:
            pl.when(cond)(body)

    def rows(index):
        return pl.ds(pl.multiple_of(index * T, 16), T)

    def copy(name, index, src, dst, to, out=None):
        at = offsets[name] + index
        return pltpu.make_async_remote_copy(
            src_ref=src,
            dst_ref=dst,
            send_sem=send_sems.at[at if out is None else offsets[name] + out],
            recv_sem=recv_sems.at[at],
            device_id=to,
            device_id_type=MESH,
        )

    def send(cond, name, index, src, dst, to, out=None):
        when(cond, lambda: copy(name, index, src(), dst(), to, out).start())
        sent.append((cond, name, index, src, dst, to, out))

    def drain(entries):
        for entry in entries:
            cond, name, index, src, dst, to, out = entry
            when(
                cond,
                lambda name=name, index=index, src=src, dst=dst, to=to, out=out: copy(
                    name, index, src(), dst(), to, out
                ).wait_send(),
            )
        done = [id(entry) for entry in entries]
        sent[:] = [entry for entry in sent if id(entry) not in done]

    def arrive(cond, name, index, dst):
        when(cond, lambda: copy(name, index, dst(), dst(), to_peer).wait_recv())

    barrier = pltpu.get_barrier_semaphore()
    for cond, to in (
        (always, to_x),
        (always, to_y),
        (always, to_diag),
        (always, to_peer),
    ) + tuple((z != k, (s, k, core)) for k in range(nz)):
        when(
            cond,
            lambda to=to: pl.semaphore_signal(
                barrier, inc=1, device_id=to, device_id_type=MESH
            ),
        )
    reads = [
        pltpu.make_async_copy(src, dst, load_sems.at[4 + nz + i])
        for i, (src, dst) in enumerate(
            (
                (fg_hbm, fg_ref),
                (ef_hbm, ef_ref),
                (ig_hbm, ig_ref),
                (k_hbm, k_ref),
                (v_hbm, v_ref),
                (q_hbm, q_ref),
                (og_hbm, og_ref),
                (hg_hbm, hg_ref),
                (gain_hbm, gain_ref),
                (routes_hbm, routes_ref),
                (choice_hbm, choice_ref),
            )
        )
    ]
    for read in reads[:5]:
        read.start()
    zcols = pl.ds(pl.multiple_of(z * wide, 128), wide)
    load_mix = pltpu.make_async_copy(mix_hbm, wown, load_sems.at[3])
    load_res = [
        pltpu.make_async_copy(
            res_hbm.at[pl.ds(pl.multiple_of((k * 2 + core) * T, 16), T), zcols],
            res.at[k],
            load_sems.at[4 + k],
        )
        for k in range(nz)
    ]
    loads = [
        pltpu.make_async_copy(src, dst.at[0], load_sems.at[i])
        for i, (src, dst) in enumerate(((gate_hbm, wg), (up_hbm, wu), (down_hbm, wd)))
    ]
    load_mix.start()
    for load in reads[5:] + load_res + loads:
        load.start()

    length = q_ref.shape[0]
    heads = q_ref.shape[1] // HEAD_DIM
    scale = HEAD_DIM ** (-0.5)
    above = lax.broadcasted_iota(jnp.int32, (length, length), 0)
    along = lax.broadcasted_iota(jnp.int32, (length, length), 1)
    for read in reads[:3]:
        read.wait()
    forget_log = jax.nn.log_sigmoid(fg_ref[...]) + ef_ref[...]
    stacked = jnp.concatenate(
        [jnp.broadcast_to(forget_log[h : h + 1], (8, length)) for h in range(heads)], axis=0
    )
    running = jnp.dot(
        stacked,
        (above <= along).astype(F32),
        precision=HIGHEST,
        preferred_element_type=F32,
    )

    def head(ref, h):
        return ref[:, h * HEAD_DIM : (h + 1) * HEAD_DIM]

    runs = [running[8 * h : 8 * h + 1] for h in range(heads)]
    for read in reads[3:5]:
        read.wait()
    for h in range(heads):
        total = runs[h][:, length - 1 :]
        log_write = ig_ref[h : h + 1, :] + total - runs[h]
        stab = jnp.max(log_write, axis=1, keepdims=True)
        write = jnp.exp(log_write - stab) * scale
        high, low = halves(jnp.transpose(head(k_ref, h).astype(F32)) * write)
        value = head(v_ref, h)
        cell = jnp.dot(high, value, preferred_element_type=F32) + jnp.dot(
            low, value, preferred_element_type=F32
        )
        cells[0, h] = cell.astype(BF16)
        marks[0, h : h + 1, :] = jnp.broadcast_to(stab, (1, HEAD_DIM))
        marks[0, heads + h : heads + h + 1, :] = jnp.broadcast_to(total, (1, HEAD_DIM))

    pl.semaphore_wait(barrier, 4 + nz - 1)

    quarter = wown.shape[0] // 4
    part_rows = quarter // 2

    def wblk(k, q, first, count):
        at = pl.ds(pl.multiple_of(q * quarter + first, 16), count)
        return lambda: wz.at[k, core, at, :]

    load_mix.wait()
    at_s = pl.ds(pl.multiple_of(s * quarter, 16), quarter)
    for d in range(1, nz):
        for cond, k in ((z + d < nz, z + d), (z >= d, z - d)):
            send(
                cond,
                "WZ",
                z,
                lambda k=k: wown.at[at_s, pl.ds(pl.multiple_of(k * wide, 128), wide)],
                wblk(z, s, 0, quarter),
                (s, k, core),
                out=k,
            )

    square_of = (("X", 1, to_x), ("Y", 2, to_y), ("D", 3, to_diag))
    for way, r, to in square_of:
        send(always, "S" + way, 0, lambda: marks.at[0], lambda r=r: marks.at[r], to)
        send(always, "C" + way, 0, lambda: cells.at[0], lambda r=r: cells.at[r], to)
    send(always, "WP", z, lambda: wown.at[:, zcols], lambda: wz.at[z, core], to_peer)
    wz[z, core] = wown[:, zcols]

    for read in reads[5:]:
        read.wait()
    for h in range(heads):
        column = lanes(runs[h])
        ahead = ig_ref[h : h + 1, :] - runs[h]
        log_inner = jnp.where(
            above >= along,
            jnp.concatenate([column] * (length // HEAD_DIM), axis=1) + ahead,
            floor_neg,
        )
        inner_max = jnp.max(log_inner, axis=1, keepdims=True)
        products = lax.dot_general(
            head(q_ref, h),
            head(k_ref, h),
            (((1,), (1,)), ((), ())),
            preferred_element_type=F32,
        )
        high, low = halves(products * (scale * jnp.exp(log_inner - inner_max)))
        value = head(v_ref, h)
        inner_ref[h] = jnp.dot(high, value, preferred_element_type=F32) + jnp.dot(
            low, value, preferred_element_type=F32
        )
        imax_ref[h] = jnp.broadcast_to(inner_max, (length, HEAD_DIM))
        rcol_ref[h] = column

    def sides(d):
        return ((z >= d, z - d, "u"), (z + d < nz, z + d, "d"))

    def w_spread(d):
        for cond, k, _ in sides(d):
            arrive(cond, "WZ", k, wblk(k, s, 0, quarter))
            send(cond, "WX", k, wblk(k, s, 0, quarter), wblk(k, s, 0, quarter), to_x)
            send(cond, "WY", k, wblk(k, s, 0, quarter), wblk(k, s, 0, quarter), to_y)

    for e in range(4):
        given = jnp.where(routes_ref[...] == e, choice_ref[...], 0.0)
        tgs[0, e : e + 1, :] = jnp.sum(given, axis=0, keepdims=True)
    for way, r, to in square_of:
        send(always, "R" + way + "1", 0, lambda: tgs.at[0], lambda r=r: tgs.at[r], to)

    for way, r, to in square_of:
        arrive(always, "S" + way, 0, lambda r=r: marks.at[r])
        arrive(always, "C" + way, 0, lambda r=r: cells.at[r])
    for h in range(heads):
        stabs = [marks[s ^ g, h : h + 1, :] for g in range(4)]
        totals = [marks[s ^ g, heads + h : heads + h + 1, :] for g in range(4)]
        levels = []
        before = jnp.zeros((1, HEAD_DIM), F32)
        for g in reversed(range(4)):
            levels.insert(0, jnp.where(g < s, stabs[g] + before, floor_neg))
            before = before + jnp.where(g < s, totals[g], 0.0)
        start_stab = before
        for level in levels:
            start_stab = jnp.maximum(start_stab, level)
        start_cell = jnp.zeros((HEAD_DIM, HEAD_DIM), F32)
        for g in range(4):
            mixing = jnp.exp(levels[g] - start_stab)
            start_cell = start_cell + jnp.where(
                g < s, mixing * cells[s ^ g, h].astype(F32), 0.0
            )
        high, low = halves(start_cell)
        query = head(q_ref, h)
        carry = jnp.dot(query, high, preferred_element_type=F32) + jnp.dot(
            query, low, preferred_element_type=F32
        )
        carried = rcol_ref[h] + start_stab
        stab_row = jnp.maximum(carried, imax_ref[h])
        numer = (
            jnp.exp(imax_ref[h] - stab_row) * inner_ref[h] + jnp.exp(carried - stab_row) * carry
        )
        normed = (
            numer
            * lax.rsqrt(jnp.mean(numer * numer, axis=1, keepdims=True) + norm_eps)
            * hg_ref[:, h * HEAD_DIM : (h + 1) * HEAD_DIM]
        )
        mixed = (jax.nn.sigmoid(head(og_ref, h).astype(F32)) * normed).astype(BF16)
        for b in range(2 * nz):
            cell_ref[b // 2, b % 2, :, h * HEAD_DIM : (h + 1) * HEAD_DIM] = mixed[
                b * T : (b + 1) * T
            ]

    def ce_send(way, k, j, cond):
        go, to = (has_up, to_up) if way == "u" else (has_down, to_down)
        go = go if cond is None else cond & go
        block = lambda: ce.at[k, (core + j) % 2]
        out = 2 * nz + j if cond is None and way == "d" else None
        send(go, "CE", k * 2 + j, block, block, to, out=out)

    send(always, "MT", 0, lambda: cell_ref.at[:, 1 - core], lambda: ce.at[z, core], to_peer)
    ce[z, core] = cell_ref[:, core]
    ce_send("u", z, 0, always)
    ce_send("d", z, 0, always)
    arrive(always, "MT", 0, lambda: ce.at[z, 1 - core])
    ce_send("u", z, 1, always)
    ce_send("d", z, 1, always)
    for d in range(1, nz):
        w_spread(d)
    ends = jnp.logical_not(has_up & has_down)

    def w_relay(d, also):
        for cond, k, _ in sides(d):
            cond = cond & also
            arrive(cond, "WX", k, wblk(k, s ^ 1, 0, quarter))
            top = wblk(k, s ^ 1, 0, part_rows)
            send(cond, "W3A", k, top, top, to_y)
            arrive(cond, "WY", k, wblk(k, s ^ 2, 0, quarter))
            low = wblk(k, s ^ 2, part_rows, part_rows)
            send(cond, "W3B", k, low, low, to_x)

    for d in range(1, nz):
        if d > 1:
            w_relay(d, ends)
        for j in range(2):
            for cond, k, way in sides(d):
                arrive(cond, "CE", k * 2 + j, lambda k=k, j=j: ce.at[k, (core + j) % 2])
                ce_send(way, k, j, cond)
        if d > 1:
            w_relay(d, has_up & has_down)
        else:
            w_relay(d, z >= 0)
    for d in range(1, nz):
        for cond, k, _ in sides(d):
            arrive(cond, "W3A", k, wblk(k, s ^ 3, 0, part_rows))
            arrive(cond, "W3B", k, wblk(k, s ^ 3, part_rows, part_rows))
            whole = lambda k=k: wz.at[k, core]
            send(cond, "WP", k, whole, whole, to_peer)
    for load in load_res:
        load.wait()
    for k in range(nz):
        arrive(always, "WP", k, lambda k=k: wz.at[k, 1 - core])
    share = wz.shape[2]
    step = min(512, wide)

    @pl.loop(0, wide // step)
    def _(n):
        cols = pl.ds(pl.multiple_of(n * step, step), step)
        total = res[:, :, cols].reshape(rows_all, step).astype(F32)
        for k in range(nz):
            for c in range(2):
                total = total + jnp.dot(
                    ce[k, c].reshape(rows_all, share),
                    wz[k, c, :, cols],
                    preferred_element_type=F32,
                )
        after_ref[:, cols] = total.astype(BF16)

    values = after_ref[...].astype(F32)
    X[0, z] = (values * gain_ref[:, zcols]).astype(BF16)

    def row_sums():
        square = values * values
        room = squares.shape[2] - rows_all
        square = jnp.concatenate([square, jnp.zeros((room, wide), F32)], axis=0)
        ones = jnp.ones((8, wide), BF16)
        dims = (((1,), (1,)), ((), ()))
        return sum(
            lax.dot_general(ones, piece, dims, preferred_element_type=F32)
            for piece in halves(square)
        )

    def xblk(r, zs, cols):
        return lambda: X.at[r, zs, :, cols]

    def z_p(way, zs, cond):
        go, to = (has_up, to_up) if way == "u" else (has_down, to_down)
        go = go if cond is None else cond & go
        out = nz if cond is None and way == "d" else None
        send(go, "PZ", zs, xblk(0, zs, colGP), xblk(0, zs, colGP), to, out=out)

    def z_q(way, r, zs, cond):
        go, to = (has_up, to_up) if way == "u" else (has_down, to_down)
        go = go if cond is None else cond & go
        out = 4 * nz + r if cond is None and way == "d" else None
        send(go, "QZ", r * nz + zs, xblk(r, zs, colGQ), xblk(r, zs, colGQ), to, out=out)

    def xy_p(cond, zs):
        send(cond, "PX", zs, xblk(0, zs, colGP), xblk(1, zs, colGP), to_x)
        send(cond, "PY", zs, xblk(0, zs, colGP), xblk(2, zs, colGP), to_y)

    send(always, "QX", 0, xblk(0, z, colGQ), xblk(1, z, colGQ), to_x)
    send(always, "QY", 0, xblk(0, z, colGQ), xblk(2, z, colGQ), to_y)
    z_p("u", z, always)
    z_p("d", z, always)
    xy_p(always, z)
    z_q("u", 0, z, always)
    z_q("d", 0, z, always)
    for load, name, buf in zip(loads, ("G", "U", "W"), (wg, wu, wd)):
        load.wait()
        send(always, name, 0, lambda buf=buf: buf.at[0], lambda buf=buf: buf.at[1], to_peer)

    for way, r, to in square_of:
        arrive(always, "R" + way + "1", 0, lambda r=r: tgs.at[r])
    for r in range(4):
        column = lanes(tgs[r, pl.ds(s, 1), :])
        for b in range(2 * nz):
            wcol_ref[b] = column[b * T : (b + 1) * T]
        for b in range(nz):
            weight_ref[r, b * T : (b + 1) * T, :] = wcol_ref[2 * b + core]

    squares[z] = row_sums()
    for k in range(nz):
        send(
            z != k,
            "SQ",
            z,
            lambda: squares.at[z],
            lambda: squares.at[z],
            (s, k, core),
            out=k,
        )
    arrive(always, "QX", 0, xblk(1, z, colGQ))
    send(always, "Q3A", 0, xblk(1, z, colGQ), xblk(3, z, colGQ), to_y)
    arrive(always, "QY", 0, xblk(2, z, colGQ))

    for d in range(1, nz):
        for cond, zs, way in sides(d):
            arrive(cond, "PZ", zs, xblk(0, zs, colGP))
            z_p(way, zs, cond)
            xy_p(cond, zs)
        if d == 1:
            z_q("u", 1, z, always)
            z_q("d", 1, z, always)
        if d == min(2, nz - 1):
            z_q("u", 2, z, always)
            z_q("d", 2, z, always)
            arrive(always, "Q3A", 0, xblk(3, z, colGQ))
            z_q("u", 3, z, always)
            z_q("d", 3, z, always)

    def diagonal(cond, zs):
        odd = [zs % 2 == i if cond is None else cond & (zs % 2 == i) for i in range(2)]
        arrive(cond, "PX", zs, xblk(1, zs, colGP))
        for i in range(2):
            cols = diag_cols(i)[0]
            send(odd[i], "P3A", zs, xblk(1, zs, cols), xblk(3, zs, cols), to_y)
        arrive(cond, "PY", zs, xblk(2, zs, colGP))
        for i in range(2):
            cols = diag_cols(i)[1]
            send(odd[i], "P3B", zs, xblk(2, zs, cols), xblk(3, zs, cols), to_x)

    def q_forward(r, d):
        for cond, zs, way in sides(d):
            go = has_up if way == "u" else has_down
            arrive(cond & go, "QZ", r * nz + zs, xblk(r, zs, colGQ))
            z_q(way, r, zs, cond)

    def q_rest(r):
        for d in range(1, nz):
            for cond, zs, way in sides(d):
                stop = jnp.logical_not(has_up if way == "u" else has_down)
                arrive(cond & stop, "QZ", r * nz + zs, xblk(r, zs, colGQ))

    forwards = sorted(
        [(r, d) for r in range(4) for d in range(1, nz - 1)],
        key=lambda at: (at[0] + 2 * at[1], -at[1]),
    )
    share = len(forwards) / (nz - 1)
    diagonal(always, z)
    for k in range(nz):
        arrive(z != k, "SQ", k, lambda k=k: squares.at[k])
    mean = sum(squares[k] for k in range(nz)) / width
    roots[0] = lax.rsqrt(mean + norm_eps)
    for way, r, to in square_of:
        send(always, "T" + way, 0, lambda: roots.at[0], lambda r=r: roots.at[r], to)
    for d in range(1, nz):
        for r, far_d in forwards[round((d - 1) * share) : round(d * share)]:
            q_forward(r, far_d)
        for cond, zs, way in sides(d):
            diagonal(cond, zs)
    for name, buf in zip(("G", "U", "W"), (wg, wu, wd)):
        arrive(always, name, 0, lambda buf=buf: buf.at[1])

    def compute(r):
        q_rest(r)
        if r == 3:
            for k in range(nz):
                arrive(always, "P3A", k, xblk(3, k, diag_cols(k % 2)[0]))
                arrive(always, "P3B", k, xblk(3, k, diag_cols(k % 2)[1]))

        if r:
            way = ("X", "Y", "D")[r - 1]
            arrive(always, "T" + way, 0, lambda: roots.at[r])
        root = lanes(roots[r][:1])[:rows_all, :1]

        @pl.loop(0, 2)
        def _(n):
            def project(matrix):
                return root * sum(
                    jnp.dot(
                        X[r, k],
                        matrix[n, k * wide : (k + 1) * wide, :],
                        preferred_element_type=F32,
                    )
                    for k in range(nz)
                )

            act[n] = (jax.nn.silu(project(wg)) * project(wu)).astype(BF16)

        @pl.loop(0, nz)
        def _(n):
            cols = pl.ds(pl.multiple_of(n * wide, wide), wide)
            total = jnp.dot(act[0], wd[0, :, cols], preferred_element_type=F32) + jnp.dot(
                act[1], wd[1, :, cols], preferred_element_type=F32
            )
            total = total * weight_ref[r][:, :1]
            if r == 0:
                total = total + jnp.where(n == z, after_ref[...].astype(F32), 0.0)
            part[r, :, cols] = total.astype(BF16)

    def far(k):
        def one(a):
            low = (a - k - 1 + nz) // nz
            return low * (nz - 1 - k) + (1 - low) * (k - a)

        high = z // (nz // 2)
        return (1 - high) * one(nz - 1 - z) + high * (nz - 1 - one(z))

    order = [far(k) for k in range(nz)]

    def pblk(r, zd, cols):
        return lambda: part.at[r, rows(zd), cols]

    def lblk(buf, zd, cols):
        return lambda: buf.at[rows(zd), cols]

    def add(r, zd, cols, *others):
        total = part[r, rows(zd), cols].astype(F32)
        for buf in others:
            total = total + buf[rows(zd), cols].astype(F32)
        part[r, rows(zd), cols] = total.astype(BF16)

    def t_send(cond, r, zd, way, last):
        buf, to = (QB, to_up) if way == "u" else (QA, to_down)
        at = 4 * nz + r if last and way == "d" else r * nz + zd
        send(cond, "TZ", at, pblk(r, zd, colQ), lambda: buf.at[r, rows(zd), :], to)

    def t_take(r, zd, way, last=False):
        buf = QB if way == "u" else QA
        ref = buf.at[r, rows(zd), :]
        at = 4 * nz + r if last and way == "d" else r * nz + zd
        copy("TZ", at, ref, ref, to_peer).wait_recv()
        part[r, rows(zd), colQ] = (
            part[r, rows(zd), colQ].astype(F32) + buf[r, rows(zd), :].astype(F32)
        ).astype(BF16)

    def t_hop(r, h):
        low, high = z == h, z == nz - 1 - h
        for zd in reversed(range(h + 1, nz)):
            if h:
                pl.when(low)(lambda zd=zd: t_take(r, zd, "u"))
            t_send(low, r, zd, "u", zd == h + 1)
        for zd in range(nz - 1 - h):
            if h:
                pl.when(high)(lambda zd=zd: t_take(r, zd, "d"))
            t_send(high, r, zd, "d", zd == nz - 2 - h)

    def t_own(r):
        pl.when(has_down)(lambda: t_take(r, z, "u", True))
        pl.when(has_up)(lambda: t_take(r, z, "d", True))

    def x_direct(k):
        zd = order[k]
        send(always, "XB", zd, pblk(1, zd, colB), lblk(LX, zd, colB), to_x)

    def y_direct(k):
        zd = order[k]
        send(always, "YA", zd, pblk(2, zd, colA), lblk(LY, zd, colA), to_y)

    def issue(k):
        zd = order[k]
        if 0 < k < nz - 1:
            x_direct(k)
            y_direct(k)
        arrive(always, "RY", zd, lblk(R, zd, colA))
        add(1, zd, colA, R)
        send(always, "XA", zd, pblk(1, zd, colA), lblk(LX, zd, colA), to_x)
        arrive(always, "RX", zd, lblk(R, zd, colB))
        add(2, zd, colB, R)
        send(always, "YB", zd, pblk(2, zd, colB), lblk(LY, zd, colB), to_y)

    def down_slot(zd, steps):
        last = 1 - (steps + nz - 1) // nz
        return zd + (nz - zd) * last

    def s_send(cond, zd, way):
        buf, to = (ZB, to_up) if way == "u" else (ZA, to_down)
        at = zd if way == "u" else down_slot(zd, z - 1 - zd)
        send(cond, "SZ", at, pblk(0, zd, colP), lblk(buf, zd, colP), to)

    def square(k):
        zd = order[k]
        arrive(always, "XB", zd, lblk(LX, zd, colB))
        arrive(always, "YA", zd, lblk(LY, zd, colA))
        arrive(always, "XA", zd, lblk(LX, zd, colA))
        arrive(always, "YB", zd, lblk(LY, zd, colB))
        add(0, zd, colP, LX, LY)
        s_send((zd > z) & jnp.logical_not(has_down), zd, "u")
        s_send((zd < z) & jnp.logical_not(has_up), zd, "d")

    def line(k):
        zd = order[k]
        up_in, down_in = (zd >= z) & has_down, (zd <= z) & has_up
        arrive(up_in, "SZ", zd, lblk(ZB, zd, colP))
        when(up_in, lambda: add(0, zd, colP, ZB))
        arrive(down_in, "SZ", down_slot(zd, z - zd), lblk(ZA, zd, colP))
        when(down_in, lambda: add(0, zd, colP, ZA))
        s_send((zd > z) & has_down, zd, "u")
        s_send((zd < z) & has_up, zd, "d")

    def q_direct():
        send(always, "TXB", 0, pblk(1, z, colQB), lblk(LX, z, colQB), to_x)
        send(always, "TYA", 0, pblk(2, z, colQA), lblk(LY, z, colQA), to_y)
        send(always, "TRY", 0, pblk(3, z, colQA), lblk(R, z, colQA), to_y)
        send(always, "TRX", 0, pblk(3, z, colQB), lblk(R, z, colQB), to_x)

    def q_relay():
        arrive(always, "TRY", 0, lblk(R, z, colQA))
        add(1, z, colQA, R)
        send(always, "TXA", 0, pblk(1, z, colQA), lblk(LX, z, colQA), to_x)
        arrive(always, "TRX", 0, lblk(R, z, colQB))
        add(2, z, colQB, R)
        send(always, "TYB", 0, pblk(2, z, colQB), lblk(LY, z, colQB), to_y)

    hops = [[(r - h, h) for h in range(nz - 1) if 0 <= r - h < 4] for r in range(4 + nz - 2)]
    drain([entry for entry in sent if entry[1] in FIRST])
    def relay(k):
        zd = order[k]
        send(always, "RY", zd, pblk(3, zd, colA), lblk(R, zd, colA), to_y)
        send(always, "RX", zd, pblk(3, zd, colB), lblk(R, zd, colB), to_x)

    for r in range(4):
        compute(r)
        if r == 1:
            x_direct(0)
        if r == 2:
            y_direct(0)
        if r == 3:
            relay(0)
            relay(1)
        for group, h in hops[r]:
            t_hop(group, h)
    early = list(sent)
    for k in range(nz - 1):
        issue(k)
        if k + 2 < nz:
            relay(k + 2)
        if 4 + k < len(hops):
            for group, h in hops[4 + k]:
                t_hop(group, h)
    square(0)
    for r in range(4):
        t_own(r)
    q_direct()
    x_direct(nz - 1)
    y_direct(nz - 1)
    for k in range(1, nz - 1):
        square(k)
        line(k - 1)
        if k == 1:
            issue(nz - 1)
    line(nz - 2)
    q_relay()
    drain(early)
    arrive(always, "TXB", 0, lblk(LX, z, colQB))
    arrive(always, "TYA", 0, lblk(LY, z, colQA))
    arrive(always, "TXA", 0, lblk(LX, z, colQA))
    arrive(always, "TYB", 0, lblk(LY, z, colQB))
    out_ref[:, colQ] = (
        part[0, rows(z), colQ].astype(F32)
        + LX[rows(z), colQ].astype(F32)
        + LY[rows(z), colQ].astype(F32)
    ).astype(BF16)
    square(nz - 1)
    line(nz - 1)
    out_ref[:, colP] = part[0, rows(z), colP]
    drain(list(sent))


def whole_layer(operands, tokens, nz):
    width = operands[11].shape[1]
    length, share = operands[0].shape
    heads = share // HEAD_DIM
    hidden = operands[13].shape[1]
    picks = operands[9].shape[0]
    rows = nz * tokens
    late = width - expert_cuts(width)[1]
    wide = width // nz
    room = (rows + HEAD_DIM - 1) // HEAD_DIM * HEAD_DIM
    _, count = semaphore_slots(nz)
    vmem, hbm = pl.BlockSpec(memory_space=pltpu.VMEM), pl.BlockSpec(memory_space=pltpu.HBM)
    plane = pltpu.VMEM((rows, width), BF16)
    side = pltpu.VMEM((4, rows, late), BF16)
    local_head = pltpu.VMEM((heads, length, HEAD_DIM), F32)
    return pl.pallas_call(
        functools.partial(layer_kernel, nz),
        out_shape=jax.ShapeDtypeStruct((tokens, width), BF16),
        in_specs=[hbm] * len(operands),
        out_specs=vmem,
        scratch_shapes=[
            *[pltpu.VMEM((length, share), BF16)] * 4,
            *[pltpu.VMEM((heads, length), F32)] * 3,
            pltpu.VMEM((1, share), F32),
            pltpu.VMEM((1, width), F32),
            pltpu.VMEM((picks, length), jnp.int32),
            pltpu.VMEM((picks, length), F32),
            pltpu.VMEM((rows, wide), BF16),
            pltpu.VMEM((4, heads, HEAD_DIM, HEAD_DIM), BF16),
            pltpu.VMEM((4, 8, HEAD_DIM), F32),
            pltpu.VMEM((4, 8, length), F32),
            local_head,
            local_head,
            local_head,
            pltpu.VMEM((nz, 2, tokens, share), BF16),
            pltpu.VMEM((nz, 2, nz, tokens, share), BF16),
            pltpu.VMEM((2 * nz, tokens, HEAD_DIM), F32),
            pltpu.VMEM((4, rows, HEAD_DIM), F32),
            pltpu.VMEM((share, width), BF16),
            pltpu.VMEM((nz, 2, share, wide), BF16),
            pltpu.VMEM((nz, tokens, wide), BF16),
            pltpu.VMEM((nz, 8, room), F32),
            pltpu.VMEM((4, 8, room), F32),
            pltpu.VMEM((4, nz, rows, wide), BF16),
            pltpu.VMEM((4, rows, width), BF16),
            plane,
            plane,
            plane,
            plane,
            plane,
            side,
            side,
            pltpu.VMEM((2, width, hidden), BF16),
            pltpu.VMEM((2, width, hidden), BF16),
            pltpu.VMEM((2, hidden, width), BF16),
            pltpu.VMEM((2, rows, hidden), BF16),
            pltpu.SemaphoreType.DMA((count,)),
            pltpu.SemaphoreType.DMA((count,)),
            pltpu.SemaphoreType.DMA((15 + nz,)),
        ],
        compiler_params=pltpu.CompilerParams(
            collective_id=1, has_side_effects=True, vmem_limit_bytes=63 * 2**20
        ),
        name="layer",
    )(*operands)


def local(
    queries,
    cell_key_rows,
    cell_value_rows,
    output_gate_logits,
    input_gate_logs,
    forget_gate_logits,
    extra_log_forget,
    head_norm_gain,
    cell_output_matrix,
    residual,
    expert_norm_gain,
    routes,
    token_expert_weights,
    expert_gate_matrix,
    expert_up_matrix,
    expert_down_matrix,
):
    length = queries.shape[0]
    heads = queries.shape[1] // HEAD_DIM
    sp_count = lax.axis_size("sp")
    z_count = lax.axis_size("z")
    sp_index = lax.axis_index("sp")
    z_index = lax.axis_index("z")
    core = lax.axis_index("core")
    tokens = length // (z_count * 2)
    width = residual.shape[1]

    gate_own, up_own, down_own = expert_gate_matrix[0], expert_up_matrix[0], expert_down_matrix[0]
    if sp_count == 4:
        operands = (
            queries,
            cell_key_rows,
            cell_value_rows,
            output_gate_logits,
            input_gate_logs,
            forget_gate_logits,
            extra_log_forget,
            head_norm_gain[None],
            expert_norm_gain[None],
            routes.T,
            token_expert_weights.T,
            cell_output_matrix,
            residual,
            gate_own,
            up_own,
            down_own,
        )
        return whole_layer(operands, tokens, z_count)

    token_gates = jnp.sum(
        jnp.where(
            routes[None, :, :] == jnp.arange(sp_count, dtype=routes.dtype)[:, None, None],
            token_expert_weights[None],
            0.0,
        ),
        axis=2,
    )
    mix_peer = swap_cores(cell_output_matrix)

    forget_log = jax.nn.log_sigmoid(forget_gate_logits) + extra_log_forget
    running = jnp.cumsum(forget_log, axis=1)
    total = running[:, -1]
    log_write = input_gate_logs + total[:, None] - running
    stab_dev = jnp.max(log_write, axis=1)
    write = jnp.exp(log_write - stab_dev[:, None])

    def head(array, h):
        return array[:, h * HEAD_DIM : (h + 1) * HEAD_DIM]

    scale = HEAD_DIM ** (-0.5)
    cell_dev = [
        lax.dot_general(
            head(cell_key_rows, h).astype(F32) * (write[h] * scale)[:, None],
            head(cell_value_rows, h).astype(F32),
            (((0,), (0,)), ((), ())),
            precision=HIGHEST,
        )
        for h in range(heads)
    ]
    scalars = jnp.pad(jnp.concatenate([stab_dev, total])[None], ((0, 7), (0, HEAD_DIM - 2 * heads)))
    pack = jnp.concatenate(cell_dev + [scalars, token_gates.reshape(-1, HEAD_DIM)], axis=0)
    packs = lax.all_gather(pack, "sp")
    cells = packs[:, : heads * HEAD_DIM].reshape(sp_count, heads, HEAD_DIM, HEAD_DIM)
    stabs = packs[:, heads * HEAD_DIM, :heads]
    totals = packs[:, heads * HEAD_DIM, heads : 2 * heads]
    gates = packs[:, heads * HEAD_DIM + 8 :].reshape(sp_count, sp_count, length)
    gates = lax.dynamic_index_in_dim(gates, sp_index, 1, keepdims=False)

    order = jnp.arange(sp_count)
    between = (order[None, :] > order[:, None]) & (order[None, :] < sp_index)
    after = jnp.sum(jnp.where(between[:, :, None], totals[None], 0.0), axis=1)
    earlier = order < sp_index
    levels = jnp.where(earlier[:, None], stabs + after, floor_neg)
    before_total = jnp.sum(jnp.where(earlier[:, None], totals, 0.0), axis=0)
    start_stab = jnp.maximum(jnp.max(levels, axis=0), before_total)
    mixing = jnp.where(earlier[:, None], jnp.exp(levels - start_stab[None]), 0.0)
    start_cell = jnp.sum(mixing[:, :, None, None] * cells, axis=0)

    causal = jnp.tril(jnp.ones((length, length), dtype=bool))
    log_inner = jnp.where(
        causal[None],
        running[:, :, None] - running[:, None, :] + input_gate_logs[:, None, :],
        floor_neg,
    )
    inner_max = jnp.max(log_inner, axis=-1)
    carried = running + start_stab[:, None]
    stab_row = jnp.maximum(carried, inner_max)
    inner_scale = jnp.exp(inner_max - stab_row)
    carry_scale = jnp.exp(carried - stab_row)
    outs = []
    for h in range(heads):
        query = head(queries, h)
        products = lax.dot_general(
            query, head(cell_key_rows, h), (((1,), (1,)), ((), ())), preferred_element_type=F32
        )
        scores = products * (scale * jnp.exp(log_inner[h] - inner_max[h][:, None]))
        inner = jnp.dot(scores, head(cell_value_rows, h).astype(F32), precision=HIGHEST)
        carry = jnp.dot(query.astype(F32), start_cell[h], precision=HIGHEST)
        numer = inner_scale[h][:, None] * inner + carry_scale[h][:, None] * carry
        outs.append(
            numer
            * lax.rsqrt(jnp.mean(numer * numer, axis=1, keepdims=True) + norm_eps)
            * head(head_norm_gain[None], h)
        )
    cell_out = (
        jax.nn.sigmoid(output_gate_logits.astype(F32)) * jnp.concatenate(outs, axis=1)
    ).astype(BF16)

    rows = cell_out.reshape(z_count, 2, tokens, cell_out.shape[1])
    mine = lax.dynamic_index_in_dim(rows, core, 1, keepdims=False)
    theirs = swap_cores(lax.dynamic_index_in_dim(rows, 1 - core, 1, keepdims=False))
    mine = mine.reshape(z_count * tokens, -1)
    theirs = theirs.reshape(z_count * tokens, -1)
    mixed = jnp.dot(mine, cell_output_matrix, preferred_element_type=F32) + jnp.dot(
        theirs, mix_peer, preferred_element_type=F32
    )
    projected = lax.psum_scatter(mixed.astype(BF16), "z", scatter_dimension=0, tiled=True)

    start = (z_index * 2 + core) * tokens
    own_residual = lax.dynamic_slice_in_dim(residual, start, tokens, 0)
    after_mix = (own_residual.astype(F32) + projected.astype(F32)).astype(BF16)
    weight = lax.dynamic_index_in_dim(
        gates.reshape(sp_count, z_count, 2, tokens), core, 2, keepdims=False
    ).reshape(sp_count, z_count * tokens, 1)
    gate_peer, up_peer, down_peer = swap_cores(gate_own), swap_cores(up_own), swap_cores(down_own)
    values = after_mix.astype(F32)
    moe_in = (
        values
        * lax.rsqrt(jnp.mean(values * values, axis=-1, keepdims=True) + norm_eps)
        * expert_norm_gain
    ).astype(BF16)
    half = width // 2
    cuts = (slice(0, half), slice(half, width))
    pieces = []
    for cut in cuts:
        line = lax.all_gather(moe_in[:, cut], "z", axis=0, tiled=True)
        pieces.append(lax.all_gather(line, "sp", axis=0, tiled=True))

    def project(matrix):
        return sum(
            jnp.dot(pieces[i], matrix[cut], preferred_element_type=F32)
            for i, cut in enumerate(cuts)
        )

    def hidden(gate_matrix, up_matrix):
        return (jax.nn.silu(project(gate_matrix)) * project(up_matrix)).astype(BF16)

    act = jnp.concatenate([hidden(gate_own, up_own), hidden(gate_peer, up_peer)], axis=1)
    down = jnp.concatenate([down_own, down_peer], axis=0)
    moe = []
    for cut in cuts:
        term = jnp.dot(act, down[:, cut], preferred_element_type=F32) * weight.reshape(-1, 1)
        summed = lax.psum_scatter(term.astype(BF16), "sp", scatter_dimension=0, tiled=True)
        moe.append(lax.psum_scatter(summed, "z", scatter_dimension=0, tiled=True))
    moe = jnp.concatenate(moe, axis=1)
    return (after_mix.astype(F32) + moe.astype(F32)).astype(BF16)


def solution(mesh):
    fine = Mesh(
        mesh.devices.reshape(mesh.shape["sp"], mesh.shape["tp"] // 2, 2), ("sp", "z", "core")
    )
    tp = ("z", "core")
    placed = (
        P("sp", tp),
        P("sp", tp),
        P("sp", tp),
        P("sp", tp),
        P(tp, "sp"),
        P(tp, "sp"),
        P(tp, "sp"),
        P(tp),
        P(tp, None),
        P("sp", None),
        P(),
        P("sp", None),
        P("sp", None),
        P("sp", None, tp),
        P("sp", None, tp),
        P("sp", tp, None),
    )
    return jax.shard_map(
        local, mesh=fine, in_specs=placed, out_specs=P(("sp", "z", "core"), None), check_vma=False
    )
```

```python
import functools

import jax
import jax.numpy as jnp
from jax import lax
from jax.experimental import pallas as pl
from jax.experimental.pallas import tpu as pltpu
from jax.sharding import Mesh, PartitionSpec as P

HEAD_DIM = 128
floor_neg = -1e30
norm_eps = 1e-06
HIGHEST = lax.Precision.HIGHEST
F32 = jnp.float32
BF16 = jnp.bfloat16


def swap_cores(x):
    return lax.ppermute(x, "core", ((0, 1), (1, 0)))


MESH = pl.DeviceIdType.MESH


def expert_cuts(width):
    tiles = width // 128
    late = round(tiles * 9 / 32)
    early = tiles - late
    a = (early + 1) // 2 * 128
    b = early * 128
    c = b + late // 2 * 128
    return a, b, c


def halves(x):
    high = x.astype(BF16)
    return high, (x - high.astype(F32)).astype(BF16)


def lanes(row):
    return jnp.transpose(jnp.broadcast_to(row, (HEAD_DIM, row.shape[1])))


FIRST = ("WZ", "WX", "WY", "W3A", "W3B", "WP", "SQ", "CE", "MT")
FIRST += ("CX", "CY", "CD", "SX", "SY", "SD", "RX1", "RY1", "RD1")


def semaphore_slots(nz):
    first = [(n, 2 * nz) for n in FIRST[:3]] + [(n, nz) for n in FIRST[3:7]]
    first += [("CE", 2 * nz + 2)]
    first += [(n, 1) for n in FIRST[8:]]
    sums = [(n, nz) for n in ("XA", "XB", "YA", "YB", "RX", "RY")]
    sums += [("SZ", nz + 1), ("TZ", 4 * nz + 4)]
    sums += [(n, 1) for n in ("TXA", "TXB", "TYA", "TYB", "TRX", "TRY")]
    gather = [("PZ", nz + 1), ("QZ", 4 * nz + 4)]
    gather += [(n, nz) for n in ("PX", "PY", "P3A", "P3B")]
    gather += [(n, 1) for n in ("QX", "QY", "Q3A", "TX", "TY", "TD", "G", "U", "W")]
    offsets = {}

    def place(kinds, at):
        for name, count in kinds:
            offsets[name] = at
            at += count
        return at

    return offsets, place(gather, max(place(first, 0), place(sums, 0)))


def layer_kernel(
    nz,
    q_hbm,
    k_hbm,
    v_hbm,
    og_hbm,
    ig_hbm,
    fg_hbm,
    ef_hbm,
    hg_hbm,
    gain_hbm,
    routes_hbm,
    choice_hbm,
    mix_hbm,
    res_hbm,
    gate_hbm,
    up_hbm,
    down_hbm,
    out_ref,
    q_ref,
    k_ref,
    v_ref,
    og_ref,
    ig_ref,
    fg_ref,
    ef_ref,
    hg_ref,
    gain_ref,
    routes_ref,
    choice_ref,
    after_ref,
    cells,
    marks,
    tgs,
    inner_ref,
    imax_ref,
    rcol_ref,
    cell_ref,
    ce,
    wcol_ref,
    weight_ref,
    wown,
    wz,
    res,
    squares,
    roots,
    X,
    part,
    LX,
    LY,
    R,
    ZB,
    ZA,
    QB,
    QA,
    wg,
    wu,
    wd,
    act,
    send_sems,
    recv_sems,
    load_sems,
):
    T, width = out_ref.shape
    rows_all, wide = after_ref.shape
    gb = wide - max(1, wide // 1024) * 128
    colGP, colGQ = pl.ds(0, gb), pl.ds(gb, wide - gb)

    def diag_cols(odd):
        cut = (gb // 128 + 1 - odd) // 2 * 128
        return pl.ds(0, cut), pl.ds(cut, gb - cut)

    ca, cb, cc = expert_cuts(width)
    colA, colB, colP = pl.ds(0, ca), pl.ds(ca, cb - ca), pl.ds(0, cb)
    colQ, colQA, colQB = pl.ds(cb, width - cb), pl.ds(cb, cc - cb), pl.ds(cc, width - cc)
    subA, subB = pl.ds(0, cc - cb), pl.ds(cc - cb, width - cc)
    offsets, _ = semaphore_slots(nz)
    s, z, core = lax.axis_index("sp"), lax.axis_index("z"), lax.axis_index("core")
    to_x, to_y = (s ^ 1, z, core), (s ^ 2, z, core)
    to_up, to_down, to_peer = (s, z + 1, core), (s, z - 1, core), (s, z, 1 - core)
    to_diag = (s ^ 3, z, core)
    has_up, has_down = z < nz - 1, z > 0
    always = None
    sent = []

    def when(cond, body):
        if cond is None:
            body()
        else:
            pl.when(cond)(body)

    def rows(index):
        return pl.ds(pl.multiple_of(index * T, 16), T)

    def copy(name, index, src, dst, to, out=None):
        at = offsets[name] + index
        return pltpu.make_async_remote_copy(
            src_ref=src,
            dst_ref=dst,
            send_sem=send_sems.at[at if out is None else offsets[name] + out],
            recv_sem=recv_sems.at[at],
            device_id=to,
            device_id_type=MESH,
        )

    def send(cond, name, index, src, dst, to, out=None):
        when(cond, lambda: copy(name, index, src(), dst(), to, out).start())
        sent.append((cond, name, index, src, dst, to, out))

    def drain(entries):
        for entry in entries:
            cond, name, index, src, dst, to, out = entry
            when(
                cond,
                lambda name=name, index=index, src=src, dst=dst, to=to, out=out: copy(
                    name, index, src(), dst(), to, out
                ).wait_send(),
            )
        done = [id(entry) for entry in entries]
        sent[:] = [entry for entry in sent if id(entry) not in done]

    def arrive(cond, name, index, dst):
        when(cond, lambda: copy(name, index, dst(), dst(), to_peer).wait_recv())

    barrier = pltpu.get_barrier_semaphore()
    for cond, to in (
        (always, to_x),
        (always, to_y),
        (always, to_diag),
        (always, to_peer),
    ) + tuple((z != k, (s, k, core)) for k in range(nz)):
        when(
            cond,
            lambda to=to: pl.semaphore_signal(
                barrier, inc=1, device_id=to, device_id_type=MESH
            ),
        )
    reads = [
        pltpu.make_async_copy(src, dst, load_sems.at[4 + nz + i])
        for i, (src, dst) in enumerate(
            (
                (fg_hbm, fg_ref),
                (ef_hbm, ef_ref),
                (ig_hbm, ig_ref),
                (k_hbm, k_ref),
                (v_hbm, v_ref),
                (q_hbm, q_ref),
                (og_hbm, og_ref),
                (hg_hbm, hg_ref),
                (gain_hbm, gain_ref),
                (routes_hbm, routes_ref),
                (choice_hbm, choice_ref),
            )
        )
    ]
    for read in reads[:5]:
        read.start()
    zcols = pl.ds(pl.multiple_of(z * wide, 128), wide)
    load_mix = pltpu.make_async_copy(mix_hbm, wown, load_sems.at[3])
    load_res = [
        pltpu.make_async_copy(
            res_hbm.at[pl.ds(pl.multiple_of((k * 2 + core) * T, 16), T), zcols],
            res.at[k],
            load_sems.at[4 + k],
        )
        for k in range(nz)
    ]
    loads = [
        pltpu.make_async_copy(src, dst.at[0], load_sems.at[i])
        for i, (src, dst) in enumerate(((gate_hbm, wg), (up_hbm, wu), (down_hbm, wd)))
    ]
    load_mix.start()
    for load in reads[5:] + load_res + loads:
        load.start()

    length = q_ref.shape[0]
    heads = q_ref.shape[1] // HEAD_DIM
    scale = HEAD_DIM ** (-0.5)
    above = lax.broadcasted_iota(jnp.int32, (length, length), 0)
    along = lax.broadcasted_iota(jnp.int32, (length, length), 1)
    for read in reads[:3]:
        read.wait()
    forget_log = jax.nn.log_sigmoid(fg_ref[...]) + ef_ref[...]
    stacked = jnp.concatenate(
        [jnp.broadcast_to(forget_log[h : h + 1], (8, length)) for h in range(heads)], axis=0
    )
    running = jnp.dot(
        stacked,
        (above <= along).astype(F32),
        precision=HIGHEST,
        preferred_element_type=F32,
    )

    def head(ref, h):
        return ref[:, h * HEAD_DIM : (h + 1) * HEAD_DIM]

    runs = [running[8 * h : 8 * h + 1] for h in range(heads)]
    for read in reads[3:5]:
        read.wait()
    for h in range(heads):
        total = runs[h][:, length - 1 :]
        log_write = ig_ref[h : h + 1, :] + total - runs[h]
        stab = jnp.max(log_write, axis=1, keepdims=True)
        write = jnp.exp(log_write - stab) * scale
        high, low = halves(jnp.transpose(head(k_ref, h).astype(F32)) * write)
        value = head(v_ref, h)
        cell = jnp.dot(high, value, preferred_element_type=F32) + jnp.dot(
            low, value, preferred_element_type=F32
        )
        cells[0, h] = cell.astype(BF16)
        marks[0, h : h + 1, :] = jnp.broadcast_to(stab, (1, HEAD_DIM))
        marks[0, heads + h : heads + h + 1, :] = jnp.broadcast_to(total, (1, HEAD_DIM))

    pl.semaphore_wait(barrier, 4 + nz - 1)

    quarter = wown.shape[0] // 4
    part_rows = quarter // 2

    def wblk(k, q, first, count):
        at = pl.ds(pl.multiple_of(q * quarter + first, 16), count)
        return lambda: wz.at[k, core, at, :]

    load_mix.wait()
    for i in range(2):
        at_s = pl.ds(pl.multiple_of(s * quarter + i * part_rows, 16), part_rows)
        for d in range(1, nz):
            for cond, k in ((z + d < nz, z + d), (z >= d, z - d)):
                send(
                    cond,
                    "WZ",
                    z * 2 + i,
                    lambda k=k, at_s=at_s: wown.at[
                        at_s, pl.ds(pl.multiple_of(k * wide, 128), wide)
                    ],
                    wblk(z, s, i * part_rows, part_rows),
                    (s, k, core),
                    out=k * 2 + i,
                )

    square_of = (("X", 1, to_x), ("Y", 2, to_y), ("D", 3, to_diag))
    for way, r, to in square_of:
        send(always, "S" + way, 0, lambda: marks.at[0], lambda r=r: marks.at[r], to)
        send(always, "C" + way, 0, lambda: cells.at[0], lambda r=r: cells.at[r], to)
    send(always, "WP", z, lambda: wown.at[:, zcols], lambda: wz.at[z, core], to_peer)
    wz[z, core] = wown[:, zcols]

    for read in reads[5:]:
        read.wait()
    for h in range(heads):
        column = lanes(runs[h])
        ahead = ig_ref[h : h + 1, :] - runs[h]
        log_inner = jnp.where(
            above >= along,
            jnp.concatenate([column] * (length // HEAD_DIM), axis=1) + ahead,
            floor_neg,
        )
        inner_max = jnp.max(log_inner, axis=1, keepdims=True)
        products = lax.dot_general(
            head(q_ref, h),
            head(k_ref, h),
            (((1,), (1,)), ((), ())),
            preferred_element_type=F32,
        )
        high, low = halves(products * (scale * jnp.exp(log_inner - inner_max)))
        value = head(v_ref, h)
        inner_ref[h] = jnp.dot(high, value, preferred_element_type=F32) + jnp.dot(
            low, value, preferred_element_type=F32
        )
        imax_ref[h] = jnp.broadcast_to(inner_max, (length, HEAD_DIM))
        rcol_ref[h] = column

    def sides(d):
        return ((z >= d, z - d, "u"), (z + d < nz, z + d, "d"))

    def w_spread(d, i):
        for cond, k, _ in sides(d):
            block = wblk(k, s, i * part_rows, part_rows)
            arrive(cond, "WZ", k * 2 + i, block)
            send(cond, "WX", k * 2 + i, block, block, to_x)
            send(cond, "WY", k * 2 + i, block, block, to_y)

    for e in range(4):
        given = jnp.where(routes_ref[...] == e, choice_ref[...], 0.0)
        tgs[0, e : e + 1, :] = jnp.sum(given, axis=0, keepdims=True)
    for way, r, to in square_of:
        send(always, "R" + way + "1", 0, lambda: tgs.at[0], lambda r=r: tgs.at[r], to)

    for way, r, to in square_of:
        arrive(always, "S" + way, 0, lambda r=r: marks.at[r])
        arrive(always, "C" + way, 0, lambda r=r: cells.at[r])
    for h in range(heads):
        stabs = [marks[s ^ g, h : h + 1, :] for g in range(4)]
        totals = [marks[s ^ g, heads + h : heads + h + 1, :] for g in range(4)]
        levels = []
        before = jnp.zeros((1, HEAD_DIM), F32)
        for g in reversed(range(4)):
            levels.insert(0, jnp.where(g < s, stabs[g] + before, floor_neg))
            before = before + jnp.where(g < s, totals[g], 0.0)
        start_stab = before
        for level in levels:
            start_stab = jnp.maximum(start_stab, level)
        start_cell = jnp.zeros((HEAD_DIM, HEAD_DIM), F32)
        for g in range(4):
            mixing = jnp.exp(levels[g] - start_stab)
            start_cell = start_cell + jnp.where(
                g < s, mixing * cells[s ^ g, h].astype(F32), 0.0
            )
        high, low = halves(start_cell)
        query = head(q_ref, h)
        carry = jnp.dot(query, high, preferred_element_type=F32) + jnp.dot(
            query, low, preferred_element_type=F32
        )
        carried = rcol_ref[h] + start_stab
        stab_row = jnp.maximum(carried, imax_ref[h])
        numer = (
            jnp.exp(imax_ref[h] - stab_row) * inner_ref[h] + jnp.exp(carried - stab_row) * carry
        )
        normed = (
            numer
            * lax.rsqrt(jnp.mean(numer * numer, axis=1, keepdims=True) + norm_eps)
            * hg_ref[:, h * HEAD_DIM : (h + 1) * HEAD_DIM]
        )
        mixed = (jax.nn.sigmoid(head(og_ref, h).astype(F32)) * normed).astype(BF16)
        for b in range(2 * nz):
            cell_ref[b // 2, b % 2, :, h * HEAD_DIM : (h + 1) * HEAD_DIM] = mixed[
                b * T : (b + 1) * T
            ]

    def ce_send(way, k, j, cond):
        go, to = (has_up, to_up) if way == "u" else (has_down, to_down)
        go = go if cond is None else cond & go
        block = lambda: ce.at[k, (core + j) % 2]
        out = 2 * nz + j if cond is None and way == "d" else None
        send(go, "CE", k * 2 + j, block, block, to, out=out)

    send(always, "MT", 0, lambda: cell_ref.at[:, 1 - core], lambda: ce.at[z, core], to_peer)
    ce[z, core] = cell_ref[:, core]
    ce_send("u", z, 0, always)
    ce_send("d", z, 0, always)
    arrive(always, "MT", 0, lambda: ce.at[z, 1 - core])
    ce_send("u", z, 1, always)
    ce_send("d", z, 1, always)
    for i in range(2):
        for d in range(1, nz):
            w_spread(d, i)
    ends = jnp.logical_not(has_up & has_down)

    def w_relay(d, also):
        for cond, k, _ in sides(d):
            cond = cond & also
            top = wblk(k, s ^ 1, 0, part_rows)
            arrive(cond, "WX", k * 2, top)
            send(cond, "W3A", k, top, top, to_y)
            low = wblk(k, s ^ 2, part_rows, part_rows)
            arrive(cond, "WY", k * 2 + 1, low)
            send(cond, "W3B", k, low, low, to_x)
            arrive(cond, "WX", k * 2 + 1, wblk(k, s ^ 1, part_rows, part_rows))
            arrive(cond, "WY", k * 2, wblk(k, s ^ 2, 0, part_rows))

    def w_share(d):
        for cond, k, _ in sides(d):
            arrive(cond, "W3A", k, wblk(k, s ^ 3, 0, part_rows))
            arrive(cond, "W3B", k, wblk(k, s ^ 3, part_rows, part_rows))
            whole = lambda k=k: wz.at[k, core]
            send(cond, "WP", k, whole, whole, to_peer)

    for d in range(1, nz):
        if d > 1:
            w_relay(d, ends)
        for j in range(2):
            for cond, k, way in sides(d):
                arrive(cond, "CE", k * 2 + j, lambda k=k, j=j: ce.at[k, (core + j) % 2])
                ce_send(way, k, j, cond)
        if d > 1:
            w_relay(d, has_up & has_down)
            w_share(d - 1)
        else:
            w_relay(d, z >= 0)
    w_share(nz - 1)
    for load in load_res:
        load.wait()
    for k in range(nz):
        arrive(always, "WP", k, lambda k=k: wz.at[k, 1 - core])
    share = wz.shape[2]
    step = min(512, wide)

    @pl.loop(0, wide // step)
    def _(n):
        cols = pl.ds(pl.multiple_of(n * step, step), step)
        total = res[:, :, cols].reshape(rows_all, step).astype(F32)
        for k in range(nz):
            for c in range(2):
                total = total + jnp.dot(
                    ce[k, c].reshape(rows_all, share),
                    wz[k, c, :, cols],
                    preferred_element_type=F32,
                )
        after_ref[:, cols] = total.astype(BF16)

    values = after_ref[...].astype(F32)
    X[0, z] = (values * gain_ref[:, zcols]).astype(BF16)

    def row_sums():
        square = values * values
        room = squares.shape[2] - rows_all
        square = jnp.concatenate([square, jnp.zeros((room, wide), F32)], axis=0)
        ones = jnp.ones((8, wide), BF16)
        dims = (((1,), (1,)), ((), ()))
        return sum(
            lax.dot_general(ones, piece, dims, preferred_element_type=F32)
            for piece in halves(square)
        )

    def xblk(r, zs, cols):
        return lambda: X.at[r, zs, :, cols]

    def z_p(way, zs, cond):
        go, to = (has_up, to_up) if way == "u" else (has_down, to_down)
        go = go if cond is None else cond & go
        out = nz if cond is None and way == "d" else None
        send(go, "PZ", zs, xblk(0, zs, colGP), xblk(0, zs, colGP), to, out=out)

    def z_q(way, r, zs, cond):
        go, to = (has_up, to_up) if way == "u" else (has_down, to_down)
        go = go if cond is None else cond & go
        out = 4 * nz + r if cond is None and way == "d" else None
        send(go, "QZ", r * nz + zs, xblk(r, zs, colGQ), xblk(r, zs, colGQ), to, out=out)

    def xy_p(cond, zs):
        send(cond, "PX", zs, xblk(0, zs, colGP), xblk(1, zs, colGP), to_x)
        send(cond, "PY", zs, xblk(0, zs, colGP), xblk(2, zs, colGP), to_y)

    send(always, "QX", 0, xblk(0, z, colGQ), xblk(1, z, colGQ), to_x)
    send(always, "QY", 0, xblk(0, z, colGQ), xblk(2, z, colGQ), to_y)
    z_p("u", z, always)
    z_p("d", z, always)
    xy_p(always, z)
    z_q("u", 0, z, always)
    z_q("d", 0, z, always)
    for load, name, buf in zip(loads, ("G", "U", "W"), (wg, wu, wd)):
        load.wait()
        send(always, name, 0, lambda buf=buf: buf.at[0], lambda buf=buf: buf.at[1], to_peer)

    for way, r, to in square_of:
        arrive(always, "R" + way + "1", 0, lambda r=r: tgs.at[r])
    for r in range(4):
        column = lanes(tgs[r, pl.ds(s, 1), :])
        for b in range(2 * nz):
            wcol_ref[b] = column[b * T : (b + 1) * T]
        for b in range(nz):
            weight_ref[r, b * T : (b + 1) * T, :] = wcol_ref[2 * b + core]

    squares[z] = row_sums()
    for k in range(nz):
        send(
            z != k,
            "SQ",
            z,
            lambda: squares.at[z],
            lambda: squares.at[z],
            (s, k, core),
            out=k,
        )
    arrive(always, "QX", 0, xblk(1, z, colGQ))
    send(always, "Q3A", 0, xblk(1, z, colGQ), xblk(3, z, colGQ), to_y)
    arrive(always, "QY", 0, xblk(2, z, colGQ))

    for d in range(1, nz):
        for cond, zs, way in sides(d):
            arrive(cond, "PZ", zs, xblk(0, zs, colGP))
            z_p(way, zs, cond)
            xy_p(cond, zs)
        if d == 1:
            z_q("u", 1, z, always)
            z_q("d", 1, z, always)
        if d == min(2, nz - 1):
            z_q("u", 2, z, always)
            z_q("d", 2, z, always)
            arrive(always, "Q3A", 0, xblk(3, z, colGQ))
            z_q("u", 3, z, always)
            z_q("d", 3, z, always)

    def diagonal(cond, zs):
        odd = [zs % 2 == i if cond is None else cond & (zs % 2 == i) for i in range(2)]
        arrive(cond, "PX", zs, xblk(1, zs, colGP))
        for i in range(2):
            cols = diag_cols(i)[0]
            send(odd[i], "P3A", zs, xblk(1, zs, cols), xblk(3, zs, cols), to_y)
        arrive(cond, "PY", zs, xblk(2, zs, colGP))
        for i in range(2):
            cols = diag_cols(i)[1]
            send(odd[i], "P3B", zs, xblk(2, zs, cols), xblk(3, zs, cols), to_x)

    def q_forward(r, d):
        for cond, zs, way in sides(d):
            go = has_up if way == "u" else has_down
            arrive(cond & go, "QZ", r * nz + zs, xblk(r, zs, colGQ))
            z_q(way, r, zs, cond)

    def q_rest(r):
        for d in range(1, nz):
            for cond, zs, way in sides(d):
                stop = jnp.logical_not(has_up if way == "u" else has_down)
                arrive(cond & stop, "QZ", r * nz + zs, xblk(r, zs, colGQ))

    forwards = sorted(
        [(r, d) for r in range(4) for d in range(1, nz - 1)],
        key=lambda at: (at[0] + 2 * at[1], -at[1]),
    )
    share = len(forwards) / (nz - 1)
    diagonal(always, z)
    for k in range(nz):
        arrive(z != k, "SQ", k, lambda k=k: squares.at[k])
    mean = sum(squares[k] for k in range(nz)) / width
    roots[0] = lax.rsqrt(mean + norm_eps)
    for way, r, to in square_of:
        send(always, "T" + way, 0, lambda: roots.at[0], lambda r=r: roots.at[r], to)
    for d in range(1, nz):
        for r, far_d in forwards[round((d - 1) * share) : round(d * share)]:
            q_forward(r, far_d)
        for cond, zs, way in sides(d):
            diagonal(cond, zs)
    for name, buf in zip(("G", "U", "W"), (wg, wu, wd)):
        arrive(always, name, 0, lambda buf=buf: buf.at[1])

    def compute(r):
        q_rest(r)
        if r == 3:
            for k in range(nz):
                arrive(always, "P3A", k, xblk(3, k, diag_cols(k % 2)[0]))
                arrive(always, "P3B", k, xblk(3, k, diag_cols(k % 2)[1]))

        if r:
            way = ("X", "Y", "D")[r - 1]
            arrive(always, "T" + way, 0, lambda: roots.at[r])
        root = lanes(roots[r][:1])[:rows_all, :1]

        @pl.loop(0, 2)
        def _(n):
            def project(matrix):
                return root * sum(
                    jnp.dot(
                        X[r, k],
                        matrix[n, k * wide : (k + 1) * wide, :],
                        preferred_element_type=F32,
                    )
                    for k in range(nz)
                )

            act[n] = (jax.nn.silu(project(wg)) * project(wu)).astype(BF16)

        @pl.loop(0, nz)
        def _(n):
            cols = pl.ds(pl.multiple_of(n * wide, wide), wide)
            total = jnp.dot(act[0], wd[0, :, cols], preferred_element_type=F32) + jnp.dot(
                act[1], wd[1, :, cols], preferred_element_type=F32
            )
            total = total * weight_ref[r][:, :1]
            if r == 0:
                total = total + jnp.where(n == z, after_ref[...].astype(F32), 0.0)
            part[r, :, cols] = total.astype(BF16)

    def far(k):
        def one(a):
            low = (a - k - 1 + nz) // nz
            return low * (nz - 1 - k) + (1 - low) * (k - a)

        high = z // (nz // 2)
        return (1 - high) * one(nz - 1 - z) + high * (nz - 1 - one(z))

    order = [far(k) for k in range(nz)]

    def pblk(r, zd, cols):
        return lambda: part.at[r, rows(zd), cols]

    def lblk(buf, zd, cols):
        return lambda: buf.at[rows(zd), cols]

    def add(r, zd, cols, *others):
        total = part[r, rows(zd), cols].astype(F32)
        for buf in others:
            total = total + buf[rows(zd), cols].astype(F32)
        part[r, rows(zd), cols] = total.astype(BF16)

    def t_send(cond, r, zd, way, last):
        buf, to = (QB, to_up) if way == "u" else (QA, to_down)
        at = 4 * nz + r if last and way == "d" else r * nz + zd
        send(cond, "TZ", at, pblk(r, zd, colQ), lambda: buf.at[r, rows(zd), :], to)

    def t_take(r, zd, way, last=False):
        buf = QB if way == "u" else QA
        ref = buf.at[r, rows(zd), :]
        at = 4 * nz + r if last and way == "d" else r * nz + zd
        copy("TZ", at, ref, ref, to_peer).wait_recv()
        part[r, rows(zd), colQ] = (
            part[r, rows(zd), colQ].astype(F32) + buf[r, rows(zd), :].astype(F32)
        ).astype(BF16)

    def t_hop(r, h):
        low, high = z == h, z == nz - 1 - h
        for zd in reversed(range(h + 1, nz)):
            if h:
                pl.when(low)(lambda zd=zd: t_take(r, zd, "u"))
            t_send(low, r, zd, "u", zd == h + 1)
        for zd in range(nz - 1 - h):
            if h:
                pl.when(high)(lambda zd=zd: t_take(r, zd, "d"))
            t_send(high, r, zd, "d", zd == nz - 2 - h)

    def t_own(r):
        pl.when(has_down)(lambda: t_take(r, z, "u", True))
        pl.when(has_up)(lambda: t_take(r, z, "d", True))

    def x_direct(k):
        zd = order[k]
        send(always, "XB", zd, pblk(1, zd, colB), lblk(LX, zd, colB), to_x)

    def y_direct(k):
        zd = order[k]
        send(always, "YA", zd, pblk(2, zd, colA), lblk(LY, zd, colA), to_y)

    def issue(k):
        zd = order[k]
        if 0 < k < nz - 1:
            x_direct(k)
            y_direct(k)
        arrive(always, "RY", zd, lblk(R, zd, colA))
        add(1, zd, colA, R)
        send(always, "XA", zd, pblk(1, zd, colA), lblk(LX, zd, colA), to_x)
        arrive(always, "RX", zd, lblk(R, zd, colB))
        add(2, zd, colB, R)
        send(always, "YB", zd, pblk(2, zd, colB), lblk(LY, zd, colB), to_y)

    def down_slot(zd, steps):
        last = 1 - (steps + nz - 1) // nz
        return zd + (nz - zd) * last

    def s_send(cond, zd, way):
        buf, to = (ZB, to_up) if way == "u" else (ZA, to_down)
        at = zd if way == "u" else down_slot(zd, z - 1 - zd)
        send(cond, "SZ", at, pblk(0, zd, colP), lblk(buf, zd, colP), to)

    def square(k):
        zd = order[k]
        arrive(always, "XB", zd, lblk(LX, zd, colB))
        arrive(always, "YA", zd, lblk(LY, zd, colA))
        arrive(always, "XA", zd, lblk(LX, zd, colA))
        arrive(always, "YB", zd, lblk(LY, zd, colB))
        add(0, zd, colP, LX, LY)
        s_send((zd > z) & jnp.logical_not(has_down), zd, "u")
        s_send((zd < z) & jnp.logical_not(has_up), zd, "d")

    def line(k):
        zd = order[k]
        up_in, down_in = (zd >= z) & has_down, (zd <= z) & has_up
        arrive(up_in, "SZ", zd, lblk(ZB, zd, colP))
        when(up_in, lambda: add(0, zd, colP, ZB))
        arrive(down_in, "SZ", down_slot(zd, z - zd), lblk(ZA, zd, colP))
        when(down_in, lambda: add(0, zd, colP, ZA))
        s_send((zd > z) & has_down, zd, "u")
        s_send((zd < z) & has_up, zd, "d")

    def q_direct():
        send(always, "TXB", 0, pblk(1, z, colQB), lblk(LX, z, colQB), to_x)
        send(always, "TYA", 0, pblk(2, z, colQA), lblk(LY, z, colQA), to_y)
        send(always, "TRY", 0, pblk(3, z, colQA), lblk(R, z, colQA), to_y)
        send(always, "TRX", 0, pblk(3, z, colQB), lblk(R, z, colQB), to_x)

    def q_relay():
        arrive(always, "TRY", 0, lblk(R, z, colQA))
        add(1, z, colQA, R)
        send(always, "TXA", 0, pblk(1, z, colQA), lblk(LX, z, colQA), to_x)
        arrive(always, "TRX", 0, lblk(R, z, colQB))
        add(2, z, colQB, R)
        send(always, "TYB", 0, pblk(2, z, colQB), lblk(LY, z, colQB), to_y)

    hops = [[(r - h, h) for h in range(nz - 1) if 0 <= r - h < 4] for r in range(4 + nz - 2)]
    drain([entry for entry in sent if entry[1] in FIRST])
    def relay(k):
        zd = order[k]
        send(always, "RY", zd, pblk(3, zd, colA), lblk(R, zd, colA), to_y)
        send(always, "RX", zd, pblk(3, zd, colB), lblk(R, zd, colB), to_x)

    for r in range(4):
        compute(r)
        if r == 1:
            x_direct(0)
        if r == 2:
            y_direct(0)
        if r == 3:
            relay(0)
            relay(1)
        for group, h in hops[r]:
            t_hop(group, h)
    early = list(sent)
    for k in range(nz - 1):
        issue(k)
        if k + 2 < nz:
            relay(k + 2)
        if 4 + k < len(hops):
            for group, h in hops[4 + k]:
                t_hop(group, h)
    square(0)
    for r in range(4):
        t_own(r)
    q_direct()
    x_direct(nz - 1)
    y_direct(nz - 1)
    for k in range(1, nz - 1):
        square(k)
        line(k - 1)
        if k == 1:
            issue(nz - 1)
    line(nz - 2)
    q_relay()
    drain(early)
    arrive(always, "TXB", 0, lblk(LX, z, colQB))
    arrive(always, "TYA", 0, lblk(LY, z, colQA))
    arrive(always, "TXA", 0, lblk(LX, z, colQA))
    arrive(always, "TYB", 0, lblk(LY, z, colQB))
    out_ref[:, colQ] = (
        part[0, rows(z), colQ].astype(F32)
        + LX[rows(z), colQ].astype(F32)
        + LY[rows(z), colQ].astype(F32)
    ).astype(BF16)
    square(nz - 1)
    line(nz - 1)
    out_ref[:, colP] = part[0, rows(z), colP]
    drain(list(sent))


def whole_layer(operands, tokens, nz):
    width = operands[11].shape[1]
    length, share = operands[0].shape
    heads = share // HEAD_DIM
    hidden = operands[13].shape[1]
    picks = operands[9].shape[0]
    rows = nz * tokens
    late = width - expert_cuts(width)[1]
    wide = width // nz
    room = (rows + HEAD_DIM - 1) // HEAD_DIM * HEAD_DIM
    _, count = semaphore_slots(nz)
    vmem, hbm = pl.BlockSpec(memory_space=pltpu.VMEM), pl.BlockSpec(memory_space=pltpu.HBM)
    plane = pltpu.VMEM((rows, width), BF16)
    side = pltpu.VMEM((4, rows, late), BF16)
    local_head = pltpu.VMEM((heads, length, HEAD_DIM), F32)
    return pl.pallas_call(
        functools.partial(layer_kernel, nz),
        out_shape=jax.ShapeDtypeStruct((tokens, width), BF16),
        in_specs=[hbm] * len(operands),
        out_specs=vmem,
        scratch_shapes=[
            *[pltpu.VMEM((length, share), BF16)] * 4,
            *[pltpu.VMEM((heads, length), F32)] * 3,
            pltpu.VMEM((1, share), F32),
            pltpu.VMEM((1, width), F32),
            pltpu.VMEM((picks, length), jnp.int32),
            pltpu.VMEM((picks, length), F32),
            pltpu.VMEM((rows, wide), BF16),
            pltpu.VMEM((4, heads, HEAD_DIM, HEAD_DIM), BF16),
            pltpu.VMEM((4, 8, HEAD_DIM), F32),
            pltpu.VMEM((4, 8, length), F32),
            local_head,
            local_head,
            local_head,
            pltpu.VMEM((nz, 2, tokens, share), BF16),
            pltpu.VMEM((nz, 2, nz, tokens, share), BF16),
            pltpu.VMEM((2 * nz, tokens, HEAD_DIM), F32),
            pltpu.VMEM((4, rows, HEAD_DIM), F32),
            pltpu.VMEM((share, width), BF16),
            pltpu.VMEM((nz, 2, share, wide), BF16),
            pltpu.VMEM((nz, tokens, wide), BF16),
            pltpu.VMEM((nz, 8, room), F32),
            pltpu.VMEM((4, 8, room), F32),
            pltpu.VMEM((4, nz, rows, wide), BF16),
            pltpu.VMEM((4, rows, width), BF16),
            plane,
            plane,
            plane,
            plane,
            plane,
            side,
            side,
            pltpu.VMEM((2, width, hidden), BF16),
            pltpu.VMEM((2, width, hidden), BF16),
            pltpu.VMEM((2, hidden, width), BF16),
            pltpu.VMEM((2, rows, hidden), BF16),
            pltpu.SemaphoreType.DMA((count,)),
            pltpu.SemaphoreType.DMA((count,)),
            pltpu.SemaphoreType.DMA((15 + nz,)),
        ],
        compiler_params=pltpu.CompilerParams(
            collective_id=1, has_side_effects=True, vmem_limit_bytes=63 * 2**20
        ),
        name="layer",
    )(*operands)


def local(
    queries,
    cell_key_rows,
    cell_value_rows,
    output_gate_logits,
    input_gate_logs,
    forget_gate_logits,
    extra_log_forget,
    head_norm_gain,
    cell_output_matrix,
    residual,
    expert_norm_gain,
    routes,
    token_expert_weights,
    expert_gate_matrix,
    expert_up_matrix,
    expert_down_matrix,
):
    length = queries.shape[0]
    heads = queries.shape[1] // HEAD_DIM
    sp_count = lax.axis_size("sp")
    z_count = lax.axis_size("z")
    sp_index = lax.axis_index("sp")
    z_index = lax.axis_index("z")
    core = lax.axis_index("core")
    tokens = length // (z_count * 2)
    width = residual.shape[1]

    gate_own, up_own, down_own = expert_gate_matrix[0], expert_up_matrix[0], expert_down_matrix[0]
    if sp_count == 4:
        operands = (
            queries,
            cell_key_rows,
            cell_value_rows,
            output_gate_logits,
            input_gate_logs,
            forget_gate_logits,
            extra_log_forget,
            head_norm_gain[None],
            expert_norm_gain[None],
            routes.T,
            token_expert_weights.T,
            cell_output_matrix,
            residual,
            gate_own,
            up_own,
            down_own,
        )
        return whole_layer(operands, tokens, z_count)

    token_gates = jnp.sum(
        jnp.where(
            routes[None, :, :] == jnp.arange(sp_count, dtype=routes.dtype)[:, None, None],
            token_expert_weights[None],
            0.0,
        ),
        axis=2,
    )
    mix_peer = swap_cores(cell_output_matrix)

    forget_log = jax.nn.log_sigmoid(forget_gate_logits) + extra_log_forget
    running = jnp.cumsum(forget_log, axis=1)
    total = running[:, -1]
    log_write = input_gate_logs + total[:, None] - running
    stab_dev = jnp.max(log_write, axis=1)
    write = jnp.exp(log_write - stab_dev[:, None])

    def head(array, h):
        return array[:, h * HEAD_DIM : (h + 1) * HEAD_DIM]

    scale = HEAD_DIM ** (-0.5)
    cell_dev = [
        lax.dot_general(
            head(cell_key_rows, h).astype(F32) * (write[h] * scale)[:, None],
            head(cell_value_rows, h).astype(F32),
            (((0,), (0,)), ((), ())),
            precision=HIGHEST,
        )
        for h in range(heads)
    ]
    scalars = jnp.pad(jnp.concatenate([stab_dev, total])[None], ((0, 7), (0, HEAD_DIM - 2 * heads)))
    pack = jnp.concatenate(cell_dev + [scalars, token_gates.reshape(-1, HEAD_DIM)], axis=0)
    packs = lax.all_gather(pack, "sp")
    cells = packs[:, : heads * HEAD_DIM].reshape(sp_count, heads, HEAD_DIM, HEAD_DIM)
    stabs = packs[:, heads * HEAD_DIM, :heads]
    totals = packs[:, heads * HEAD_DIM, heads : 2 * heads]
    gates = packs[:, heads * HEAD_DIM + 8 :].reshape(sp_count, sp_count, length)
    gates = lax.dynamic_index_in_dim(gates, sp_index, 1, keepdims=False)

    order = jnp.arange(sp_count)
    between = (order[None, :] > order[:, None]) & (order[None, :] < sp_index)
    after = jnp.sum(jnp.where(between[:, :, None], totals[None], 0.0), axis=1)
    earlier = order < sp_index
    levels = jnp.where(earlier[:, None], stabs + after, floor_neg)
    before_total = jnp.sum(jnp.where(earlier[:, None], totals, 0.0), axis=0)
    start_stab = jnp.maximum(jnp.max(levels, axis=0), before_total)
    mixing = jnp.where(earlier[:, None], jnp.exp(levels - start_stab[None]), 0.0)
    start_cell = jnp.sum(mixing[:, :, None, None] * cells, axis=0)

    causal = jnp.tril(jnp.ones((length, length), dtype=bool))
    log_inner = jnp.where(
        causal[None],
        running[:, :, None] - running[:, None, :] + input_gate_logs[:, None, :],
        floor_neg,
    )
    inner_max = jnp.max(log_inner, axis=-1)
    carried = running + start_stab[:, None]
    stab_row = jnp.maximum(carried, inner_max)
    inner_scale = jnp.exp(inner_max - stab_row)
    carry_scale = jnp.exp(carried - stab_row)
    outs = []
    for h in range(heads):
        query = head(queries, h)
        products = lax.dot_general(
            query, head(cell_key_rows, h), (((1,), (1,)), ((), ())), preferred_element_type=F32
        )
        scores = products * (scale * jnp.exp(log_inner[h] - inner_max[h][:, None]))
        inner = jnp.dot(scores, head(cell_value_rows, h).astype(F32), precision=HIGHEST)
        carry = jnp.dot(query.astype(F32), start_cell[h], precision=HIGHEST)
        numer = inner_scale[h][:, None] * inner + carry_scale[h][:, None] * carry
        outs.append(
            numer
            * lax.rsqrt(jnp.mean(numer * numer, axis=1, keepdims=True) + norm_eps)
            * head(head_norm_gain[None], h)
        )
    cell_out = (
        jax.nn.sigmoid(output_gate_logits.astype(F32)) * jnp.concatenate(outs, axis=1)
    ).astype(BF16)

    rows = cell_out.reshape(z_count, 2, tokens, cell_out.shape[1])
    mine = lax.dynamic_index_in_dim(rows, core, 1, keepdims=False)
    theirs = swap_cores(lax.dynamic_index_in_dim(rows, 1 - core, 1, keepdims=False))
    mine = mine.reshape(z_count * tokens, -1)
    theirs = theirs.reshape(z_count * tokens, -1)
    mixed = jnp.dot(mine, cell_output_matrix, preferred_element_type=F32) + jnp.dot(
        theirs, mix_peer, preferred_element_type=F32
    )
    projected = lax.psum_scatter(mixed.astype(BF16), "z", scatter_dimension=0, tiled=True)

    start = (z_index * 2 + core) * tokens
    own_residual = lax.dynamic_slice_in_dim(residual, start, tokens, 0)
    after_mix = (own_residual.astype(F32) + projected.astype(F32)).astype(BF16)
    weight = lax.dynamic_index_in_dim(
        gates.reshape(sp_count, z_count, 2, tokens), core, 2, keepdims=False
    ).reshape(sp_count, z_count * tokens, 1)
    gate_peer, up_peer, down_peer = swap_cores(gate_own), swap_cores(up_own), swap_cores(down_own)
    values = after_mix.astype(F32)
    moe_in = (
        values
        * lax.rsqrt(jnp.mean(values * values, axis=-1, keepdims=True) + norm_eps)
        * expert_norm_gain
    ).astype(BF16)
    half = width // 2
    cuts = (slice(0, half), slice(half, width))
    pieces = []
    for cut in cuts:
        line = lax.all_gather(moe_in[:, cut], "z", axis=0, tiled=True)
        pieces.append(lax.all_gather(line, "sp", axis=0, tiled=True))

    def project(matrix):
        return sum(
            jnp.dot(pieces[i], matrix[cut], preferred_element_type=F32)
            for i, cut in enumerate(cuts)
        )

    def hidden(gate_matrix, up_matrix):
        return (jax.nn.silu(project(gate_matrix)) * project(up_matrix)).astype(BF16)

    act = jnp.concatenate([hidden(gate_own, up_own), hidden(gate_peer, up_peer)], axis=1)
    down = jnp.concatenate([down_own, down_peer], axis=0)
    moe = []
    for cut in cuts:
        term = jnp.dot(act, down[:, cut], preferred_element_type=F32) * weight.reshape(-1, 1)
        summed = lax.psum_scatter(term.astype(BF16), "sp", scatter_dimension=0, tiled=True)
        moe.append(lax.psum_scatter(summed, "z", scatter_dimension=0, tiled=True))
    moe = jnp.concatenate(moe, axis=1)
    return (after_mix.astype(F32) + moe.astype(F32)).astype(BF16)


def solution(mesh):
    fine = Mesh(
        mesh.devices.reshape(mesh.shape["sp"], mesh.shape["tp"] // 2, 2), ("sp", "z", "core")
    )
    tp = ("z", "core")
    placed = (
        P("sp", tp),
        P("sp", tp),
        P("sp", tp),
        P("sp", tp),
        P(tp, "sp"),
        P(tp, "sp"),
        P(tp, "sp"),
        P(tp),
        P(tp, None),
        P("sp", None),
        P(),
        P("sp", None),
        P("sp", None),
        P("sp", None, tp),
        P("sp", None, tp),
        P("sp", tp, None),
    )
    return jax.shard_map(
        local, mesh=fine, in_specs=placed, out_specs=P(("sp", "z", "core"), None), check_vma=False
    )
```
